32 devices in a mesh: sp: 8 (over z, x), tp: 4 (over y, core).
Axes of the slice: x: 2, y: 2, z: 4, core: 2. Of those that a mesh axis runs over, the one named last changes fastest.
Arguments:
- query_maps: bfloat16 [1536, 1024], P('sp', 'tp'), may hold values from -6 to 6
- key_maps: bfloat16 [1536, 512], P('sp', 'tp'), may hold values from -6 to 6
- value_rows: bfloat16 [1536, 512], P('sp', 'tp'), may hold values from -6 to 6
- mix_lambda: float32 [8], P('tp'), may hold values from 0.3 to 0.8
- head_gain: float32 [128], replicated, may hold values from 0.1 to 1.9
- out_weight: bfloat16 [1024, 2048], replicated, may hold values from -0.1875 to 0.1875
- residual: bfloat16 [1536, 2048], P(('sp', 'tp')), may hold values from -6 to 6
- norm_gain: float32 [2048], replicated, may hold values from 0.1 to 1.9
- routes: int32 [1536, 4], P('sp'), may hold values from 0 to 7, all different within a row; in each aligned block of 48 rows (0 to 47, 48 to 95, ...) at most 48 rows name the same one
- route_weight: float32 [1536, 4], P(('sp', 'tp')), may hold values from 0.3 to 1.5
- expert_gate: bfloat16 [8, 2048, 1024], P('sp', None, 'tp'), may hold values from -0.125 to 0.125
- expert_up: bfloat16 [8, 2048, 1024], P('sp', None, 'tp'), may hold values from -0.125 to 0.125
- expert_down: bfloat16 [8, 1024, 2048], P('sp', 'tp'), may hold values from -0.1875 to 0.1875
- shared_gate: bfloat16 [2048, 1024], P(None, 'tp'), may hold values from -0.125 to 0.125
- shared_up: bfloat16 [2048, 1024], P(None, 'tp'), may hold values from -0.125 to 0.125
- shared_down: bfloat16 [1024, 2048], P('tp'), may hold values from -0.1875 to 0.1875
Outputs:
- mixed: bfloat16 [1536, 2048], P(('sp', 'tp'))
The draws below stay inside these ranges and needn't reach their ends.
Inputs may be any that keep to these rules, and one draw needn't show every extreme that they name: `routes`: the 4 experts of a token are different. In each aligned block of 48 tokens (the tokens of one device after the attention) no expert is named more than 48 times, a bound that some expert reaches in some blocks.
All inputs are finite; a program needn't handle non-finite values.
Results may differ from the reference program's by a relative error of at most 0.018.
Values may be sent and summed in bfloat16 or wider, within the bound.
A program may use at most 128 MiB of HBM per device.

```python
import math
import jax
import jax.numpy as jnp
import numpy as np
from jax import lax

D = 2048
HEADS = 8
KV_HEADS = 4
HD = 64
VD = 128
EXPERTS = 8
EXP_FF = 1024
SH_FF = 1024
TOP_K = 4
SEQ = 1536
ROWS_DEV = 48
CAP = 48
N_TP = 4


def base_values(key, salt, shape):
    values = jnp.clip(1.3 * jax.random.normal(jax.random.fold_in(key, salt), shape, jnp.float32), -6.0, 6.0)
    return values


def draw_key_maps(key, part):
    values = base_values(key, 7010, (SEQ, KV_HEADS * 2 * HD))
    return values.astype(jnp.bfloat16)


def draw_query_maps(key, part):
    values = base_values(key, 7020, (SEQ, HEADS * 2 * HD))
    return values.astype(jnp.bfloat16)


def levels(own_key, extent, pieces, low, top_value):
    def one(dim, shards_of):
        heights = jax.random.uniform(jax.random.fold_in(jax.random.fold_in(own_key, 6), dim), (shards_of,), jnp.float32, low / len(pieces), top_value / len(pieces))
        return jnp.repeat(jnp.exp(heights), extent[dim] // shards_of).reshape((-1,) + (1,) * (len(extent) - dim - 1))

    factor_of = one(*pieces[0])
    for cut in pieces[1:]:
        factor_of = factor_of * one(*cut)
    return factor_of


def routed_block(own_key, own, number, rows, amount, top, bound, skew):
    sequence = jax.random.permutation(own_key, amount)
    packed, ordinary = shares(amount, rows * top, bound, skew, True), shares(amount, rows * top, bound, skew, False)
    places = jnp.arange(amount)

    def named(sizes, offset_by):
        used = int((sizes > 0).sum())
        fixed = max(1, used // 4)
        shifted = fixed + (places - fixed + offset_by * (used - fixed)) % max(1, amount - fixed)
        return jnp.zeros((amount,), jnp.int32).at[sequence[jnp.where(places < fixed, places, shifted)]].set(jnp.asarray(sizes, jnp.int32))

    sizes = jnp.where(number % 4 == 0, named(packed, number // 4), named(ordinary, number - number // 4 - 1))
    mixed = jax.random.permutation(jax.random.fold_in(own, 3), amount)
    giver, taker = mixed[0:amount // 2 * 2:2], mixed[1:amount // 2 * 2:2]
    room = jnp.minimum(sizes[giver] - 1, bound - sizes[taker]) // 2
    room = jnp.where((giver == sequence[0]) | (taker == sequence[0]) | (sizes[taker] == 0), 0, jnp.maximum(room, 0))
    shifted = jax.random.randint(jax.random.fold_in(own, 4), (amount // 2,), 0, 1 << 20) % (room + 1)
    sizes = sizes.at[giver].add(-shifted).at[taker].add(shifted)
    members = jnp.searchsorted(jnp.cumsum(sizes), jnp.arange(rows * top), side="right").astype(jnp.int32)
    grid = members.reshape(top, rows).T
    grid = grid[jax.random.permutation(jax.random.fold_in(own, 1), rows)]
    offset_by = jax.random.randint(jax.random.fold_in(own, 2), (rows, 1), 0, top)
    return jnp.take_along_axis(grid, (jnp.arange(top)[None, :] + offset_by) % top, axis=1)


def shares(count, total, most, lean, full):
    portions = [(1 << 20) // math.isqrt(standing ** lean) + 1 for standing in range(1, count + 1)]
    largest = most if full else min(most, max(-(-total // count), total * portions[0] // sum(portions)))
    least = 1 if total - largest >= count - 1 else 0
    holding, surplus = [largest] + [least] * (count - 1), total - largest - least * (count - 1)
    while surplus > 0:
        candidates = [i for i in range(1, count) if holding[i] < largest] or [i for i in range(1, count) if holding[i] < most]
        mass, left = sum([portions[i] for i in candidates]), surplus
        for i in candidates:
            more = min(most - holding[i], max(1, left * portions[i] // mass), surplus)
            holding[i] = holding[i] + more
            surplus = surplus - more
    return np.array(holding)


def bell_draw(key, dims, spread, reach, shards=(), held_as=jnp.bfloat16):
    result = jax.random.normal(key, dims, jnp.float32) * spread
    if len(shards) > 0:
        result = levels(key, dims, shards, -0.22, 0.18) * result
    return jnp.clip(result, min=-reach, max=reach).astype(held_as)


def setup_inputs(seed: int = 0) -> dict:
    arg_keys = jax.random.split(jax.random.key(seed), 17)
    query_maps = draw_query_maps(jax.random.fold_in(arg_keys[16], 71), 0)
    key_maps = draw_key_maps(jax.random.fold_in(arg_keys[16], 71), 0)
    value_rows = bell_draw(arg_keys[2], (SEQ, KV_HEADS * VD), 1.0, 6.0, ((0, 8), (1, 4)))
    mix_lambda = jnp.clip(0.3 + 0.5 * jax.random.uniform(arg_keys[3], (HEADS,), jnp.float32) ** levels(arg_keys[3], (HEADS,), ((0, 4),), -0.2, 0.2), 0.3, 0.8)
    head_gain = jnp.clip(1.0 + 0.18 * jax.random.normal(arg_keys[4], (VD,), jnp.float32), 0.1, 1.9)
    out_weight = bell_draw(arg_keys[5], (HEADS * VD, D), (HEADS * VD) ** -0.5, 0.1875)
    residual = bell_draw(arg_keys[6], (SEQ, D), 1.0, 6.0, ((0, 32),))
    norm_gain = jnp.clip(1.0 + 0.18 * jax.random.normal(arg_keys[7], (D,), jnp.float32), 0.1, 1.9)
    routes_keys = jax.random.split(jax.random.fold_in(arg_keys[8], 1), SEQ // ROWS_DEV)
    routes_turns = jax.random.permutation(jax.random.fold_in(arg_keys[8], 3), SEQ // ROWS_DEV)
    routes = jax.vmap(lambda own, number: routed_block(jax.random.fold_in(arg_keys[8], 2), own, number, ROWS_DEV, EXPERTS, TOP_K, CAP, 2))(routes_keys, routes_turns).reshape((SEQ, TOP_K))
    route_weight = jnp.clip(jnp.exp(math.log(1.5) - 1.60943787 * jax.random.uniform(arg_keys[9], (SEQ, TOP_K), jnp.float32) ** levels(arg_keys[9], (SEQ, TOP_K), ((0, 32),), -0.2, 0.2)), 0.3, 1.5)
    expert_gate = bell_draw(arg_keys[10], (EXPERTS, D, EXP_FF), D ** -0.5, 0.125, ((0, 8), (2, 4)))
    expert_up = bell_draw(arg_keys[11], (EXPERTS, D, EXP_FF), D ** -0.5, 0.125, ((0, 8), (2, 4)))
    expert_down = bell_draw(arg_keys[12], (EXPERTS, EXP_FF, D), EXP_FF ** -0.5, 0.1875, ((0, 8), (1, 4)))
    shared_gate = bell_draw(arg_keys[13], (D, SH_FF), D ** -0.5, 0.125, ((1, 4),))
    shared_up = bell_draw(arg_keys[14], (D, SH_FF), D ** -0.5, 0.125, ((1, 4),))
    shared_down = bell_draw(arg_keys[15], (SH_FF, D), SH_FF ** -0.5, 0.1875, ((0, 4),))
    return dict(query_maps=query_maps, key_maps=key_maps, value_rows=value_rows, mix_lambda=mix_lambda, head_gain=head_gain, out_weight=out_weight, residual=residual, norm_gain=norm_gain, routes=routes, route_weight=route_weight, expert_gate=expert_gate, expert_up=expert_up, expert_down=expert_down, shared_gate=shared_gate, shared_up=shared_up, shared_down=shared_down)


norm_eps = 1e-06

def slot_targets(block_routes):
    flat_routes = block_routes.reshape(-1)
    onehot = (flat_routes[:, None] == jnp.arange(EXPERTS, dtype=jnp.int32)[None, :]).astype(jnp.int32)
    earlier = jnp.cumsum(onehot, axis=0) - onehot
    return (flat_routes, lax.optimization_barrier(jnp.sum(earlier * onehot, axis=1)).astype(jnp.int32))

def grouped_feedforward(token_rows, gate_weight, up_weight, down_weight):
    gate_value = jnp.dot(token_rows, gate_weight, preferred_element_type=jnp.float32)
    up_value = jnp.dot(token_rows, up_weight, preferred_element_type=jnp.float32)
    hidden = (jax.nn.silu(gate_value) * up_value).astype(jnp.bfloat16)
    group_width = hidden.shape[1] // N_TP
    running = jnp.zeros((token_rows.shape[0], down_weight.shape[1]), jnp.float32)
    for group_index in range(N_TP):
        partial_sum = jnp.dot(hidden[:, group_index * group_width:(group_index + 1) * group_width], down_weight[group_index * group_width:(group_index + 1) * group_width], preferred_element_type=jnp.float32)
        running = running + lax.optimization_barrier(partial_sum.astype(jnp.bfloat16)).astype(jnp.float32)
    return running.astype(jnp.bfloat16)

def head_attention(query_maps, key_maps, value_rows, mix_lambda, head_gain, head_index):
    kv_index = head_index // (HEADS // KV_HEADS)
    head_query = lax.dynamic_slice_in_dim(query_maps, (head_index * 2 * HD).astype(jnp.int32), 2 * HD, 1)
    head_key = lax.dynamic_slice_in_dim(key_maps, (kv_index * 2 * HD).astype(jnp.int32), 2 * HD, 1)
    head_value = lax.dynamic_slice_in_dim(value_rows, (kv_index * VD).astype(jnp.int32), VD, 1)
    head_lambda = mix_lambda[head_index]
    score_scale = HD ** (-0.5)
    block_rows = math.gcd(SEQ, 512)
    query_blocks = head_query.reshape(SEQ // block_rows, block_rows, 2 * HD)

    def weighted(scores):
        row_max = lax.optimization_barrier(jnp.max(scores, axis=1, keepdims=True))
        exp_scores = jnp.exp(scores - row_max)
        row_total = lax.optimization_barrier(jnp.sum(exp_scores, axis=1, keepdims=True))
        return jnp.dot(exp_scores.astype(jnp.bfloat16), head_value, preferred_element_type=jnp.float32) / row_total

    def one_block(query_block):
        first_map = jnp.dot(query_block[:, :HD], head_key[:, :HD].T, preferred_element_type=jnp.float32) * score_scale
        second_map = jnp.dot(query_block[:, HD:], head_key[:, HD:].T, preferred_element_type=jnp.float32) * score_scale
        difference = weighted(first_map) - head_lambda * weighted(second_map)
        inverse_rms = lax.rsqrt(lax.optimization_barrier(jnp.mean(difference * difference, axis=1, keepdims=True)) + norm_eps)
        return (difference * inverse_rms * head_gain).astype(jnp.bfloat16)
    return lax.map(one_block, query_blocks).reshape(SEQ, VD)

def reference(query_maps, key_maps, value_rows, mix_lambda, head_gain, out_weight, residual, norm_gain, routes, route_weight, expert_gate, expert_up, expert_down, shared_gate, shared_up, shared_down):

    def per_head(head_index):
        return head_attention(query_maps, key_maps, value_rows, mix_lambda, head_gain, head_index)
    attended = lax.map(per_head, jnp.arange(HEADS, dtype=jnp.int32))
    attended = jnp.transpose(attended, (1, 0, 2)).reshape(SEQ, HEADS * VD)
    projected = jnp.dot(attended, out_weight, preferred_element_type=jnp.float32)
    stream = (residual.astype(jnp.float32) + projected).astype(jnp.bfloat16)
    stream_wide = stream.astype(jnp.float32)
    inverse_rms = lax.rsqrt(lax.optimization_barrier(jnp.mean(stream_wide * stream_wide, axis=1, keepdims=True)) + norm_eps)
    normed = (stream_wide * inverse_rms * norm_gain).astype(jnp.bfloat16)
    blocks = SEQ // ROWS_DEV
    flat_routes, slot_index = jax.vmap(slot_targets)(routes.reshape(blocks, ROWS_DEV, TOP_K))
    expert_row = jnp.arange(blocks, dtype=jnp.int32)[:, None] * CAP + slot_index
    assignment = jnp.arange(SEQ * TOP_K, dtype=jnp.int32).reshape(blocks, ROWS_DEV * TOP_K)
    holder = jnp.full((EXPERTS, blocks * CAP), SEQ * TOP_K, jnp.int32).at[flat_routes, expert_row].set(assignment)
    padded_tokens = jnp.concatenate([normed, jnp.zeros((1, D), jnp.bfloat16)], axis=0)
    padded_weights = jnp.concatenate([route_weight.reshape(-1), jnp.zeros((1,), jnp.float32)], axis=0)

    def expert_step(running, inputs):
        holder_row, gate_weight, up_weight, down_weight = inputs
        token_index = holder_row // TOP_K
        outputs = grouped_feedforward(padded_tokens[token_index], gate_weight, up_weight, down_weight)
        contribution = padded_weights[holder_row][:, None] * outputs.astype(jnp.float32)
        return (running.at[token_index].add(contribution), None)
    routed_total = lax.scan(expert_step, jnp.zeros((SEQ + 1, D), jnp.float32), (holder, expert_gate, expert_up, expert_down))[0]
    shared_out = grouped_feedforward(normed, shared_gate, shared_up, shared_down)
    return (stream_wide + shared_out.astype(jnp.float32) + routed_total[:SEQ]).astype(jnp.bfloat16)
```

```python
from functools import partial

import jax
import jax.numpy as jnp
from jax import lax
from jax.experimental import pallas as pl
from jax.experimental.pallas import tpu as pltpu
from jax.sharding import PartitionSpec as P


norm_eps = 1e-06
lowest_score = -1e30


def slot_targets(block_routes, experts, capacity):
    flat_routes = block_routes.reshape(-1)
    onehot = (flat_routes[:, None] == jnp.arange(experts, dtype=jnp.int32)[None, :]).astype(
        jnp.int32
    )
    earlier = jnp.cumsum(onehot, axis=0) - onehot
    return flat_routes * capacity + jnp.sum(earlier * onehot, axis=1)


def build_buffer(token_rows, block_routes, experts, capacity):
    targets = slot_targets(block_routes, experts, capacity)
    row_total = block_routes.shape[0]
    route_count = block_routes.shape[1]
    source_row = jnp.arange(row_total * route_count, dtype=jnp.int32) // route_count
    holder = jnp.full((experts * capacity,), row_total, jnp.int32).at[targets].set(source_row)
    padded = jnp.concatenate(
        [token_rows, jnp.zeros((1, token_rows.shape[1]), token_rows.dtype)], axis=0
    )
    return (padded[holder], targets)


def attention_block(carried, queries, key_block, value_block, score_scale):
    run_max, run_sum, accumulated = carried
    kv_local = run_max.shape[0]
    key_heads = key_block.reshape(key_block.shape[0], kv_local, 2, -1)
    value_heads = value_block.reshape(value_block.shape[0], kv_local, -1)
    scores = (
        jnp.einsum("qagcd,racd->agcqr", queries, key_heads, preferred_element_type=jnp.float32)
        * score_scale
    )
    new_max = jnp.maximum(run_max, jnp.max(scores, axis=-1))
    rescale = jnp.exp(run_max - new_max)
    weights = jnp.exp(scores - new_max[..., None])
    run_sum = run_sum * rescale + jnp.sum(weights, axis=-1)
    update = jnp.einsum(
        "agcqr,rae->agcqe",
        weights.astype(jnp.bfloat16),
        value_heads,
        preferred_element_type=jnp.float32,
    )
    return (new_max, run_sum, accumulated * rescale[..., None] + update)


def fold_keys(carried, pieces, first_row, queries, score_scale):
    key_piece, value_piece = pieces
    total_rows = key_piece.shape[0]
    block_rows = total_rows
    for candidate in (2048, 1024, 512):
        if total_rows % candidate == 0:
            block_rows = candidate
            break
    block_count = total_rows // block_rows

    def block_step(block_index, running):
        start_row = block_index * block_rows
        return attention_block(
            running,
            queries,
            lax.dynamic_slice_in_dim(key_piece, start_row, block_rows, 0),
            lax.dynamic_slice_in_dim(value_piece, start_row, block_rows, 0),
            score_scale,
        )

    return lax.fori_loop(0, block_count, block_step, carried)


def whole_experts(arrived, whole_gate, whole_up, whole_down, senders, capacity, groups):
    local_experts = whole_gate.shape[0]
    width = arrived.shape[-1]
    rows_in = arrived.reshape(senders, local_experts, capacity, width)
    gate_value = jnp.einsum(
        "sjtd,jdf->sjtf", rows_in, whole_gate, preferred_element_type=jnp.float32
    )
    up_value = jnp.einsum("sjtd,jdf->sjtf", rows_in, whole_up, preferred_element_type=jnp.float32)
    hidden = (jax.nn.silu(gate_value) * up_value).astype(jnp.bfloat16)
    hidden_units = hidden.shape[-1]
    hidden = hidden.reshape(senders, local_experts, capacity, groups, hidden_units // groups)
    down_groups = whole_down.reshape(local_experts, groups, hidden_units // groups, width)
    group_sums = jnp.einsum(
        "sjtgf,jgfd->sjtgd", hidden, down_groups, preferred_element_type=jnp.float32
    )
    group_sums = lax.optimization_barrier(group_sums.astype(jnp.bfloat16)).astype(jnp.float32)
    return (
        jnp.sum(group_sums, axis=3)
        .astype(jnp.bfloat16)
        .reshape(senders * local_experts * capacity, width)
    )


def body(
    query_maps,
    key_maps,
    value_rows,
    mix_lambda,
    head_gain,
    out_weight,
    residual,
    norm_gain,
    routes,
    route_weight,
    expert_gate,
    expert_up,
    expert_down,
    shared_gate,
    shared_up,
    shared_down,
):
    local_heads = mix_lambda.shape[0]
    head_width = head_gain.shape[0]
    kv_local = value_rows.shape[1] // head_width
    head_group = local_heads // kv_local
    head_dim = key_maps.shape[1] // (2 * kv_local)
    token_count = query_maps.shape[0]
    queries = query_maps.reshape(token_count, kv_local, head_group, 2, head_dim)
    start_max = jnp.full((kv_local, head_group, 2, token_count), lowest_score, jnp.float32)
    start_sum = jnp.zeros((kv_local, head_group, 2, token_count), jnp.float32)
    start_values = jnp.zeros((kv_local, head_group, 2, token_count, head_width), jnp.float32)
    folder = partial(fold_keys, queries=queries, score_scale=head_dim ** (-0.5))
    _, run_sum, accumulated = folder(
        (start_max, start_sum, start_values),
        (
            lax.all_gather(key_maps, "sp", axis=0, tiled=True),
            lax.all_gather(value_rows, "sp", axis=0, tiled=True),
        ),
        jnp.int32(0),
    )
    normalized = accumulated / run_sum[..., None]
    lambdas = mix_lambda.reshape(kv_local, head_group, 1, 1)
    difference = normalized[:, :, 0] - lambdas * normalized[:, :, 1]
    inverse_rms = lax.rsqrt(jnp.mean(difference * difference, axis=-1, keepdims=True) + norm_eps)
    head_scaled = (difference * inverse_rms * head_gain).astype(jnp.bfloat16)
    attended = jnp.transpose(head_scaled, (2, 0, 1, 3)).reshape(
        token_count, local_heads * head_width
    )
    columns = lax.axis_size("tp")
    column = lax.axis_index("tp")
    rows_dev = token_count // columns
    own_rows = lax.dynamic_slice_in_dim(
        out_weight, column * attended.shape[1], attended.shape[1], 0
    )
    projected = lax.psum_scatter(
        jnp.dot(attended, own_rows, preferred_element_type=jnp.float32).astype(jnp.bfloat16),
        "tp",
        scatter_dimension=0,
        tiled=True,
    ).astype(jnp.float32)
    stream = (residual.astype(jnp.float32) + projected).astype(jnp.bfloat16)
    stream_wide = stream.astype(jnp.float32)
    stream_rms = lax.rsqrt(jnp.mean(stream_wide * stream_wide, axis=1, keepdims=True) + norm_eps)
    normed = (stream_wide * stream_rms * norm_gain).astype(jnp.bfloat16)
    senders = lax.axis_size("sp")
    local_experts = expert_gate.shape[0]
    experts = senders * local_experts
    route_count = routes.shape[1]
    capacity = max(2, 2 * rows_dev * route_count // experts)
    local_routed = None
    whole_gate, whole_up, whole_down = (
        lax.all_gather(expert_gate, "tp", axis=2, tiled=True),
        lax.all_gather(expert_up, "tp", axis=2, tiled=True),
        lax.all_gather(expert_down, "tp", axis=1, tiled=True),
    )
    own_routes = lax.dynamic_slice_in_dim(routes, column * rows_dev, rows_dev, 0)
    buffer, targets = build_buffer(normed, own_routes, experts, capacity)
    arrived = lax.all_to_all(buffer, "sp", split_axis=0, concat_axis=0, tiled=True)
    local_routed = whole_experts(
        arrived, whole_gate, whole_up, whole_down, senders, capacity, columns
    )
    shared_rows = lax.all_gather(normed[None], "tp", axis=0, tiled=True)
    shared_in = shared_rows
    shared_in = shared_in.reshape(1 * lax.axis_size("tp") * rows_dev, shared_in.shape[-1])
    shared_hidden = (
        jax.nn.silu(jnp.dot(shared_in, shared_gate, preferred_element_type=jnp.float32))
        * jnp.dot(shared_in, shared_up, preferred_element_type=jnp.float32)
    ).astype(jnp.bfloat16)
    shared_out = jnp.dot(shared_hidden, shared_down, preferred_element_type=jnp.float32)
    pieces = shared_out.reshape(1 * lax.axis_size("tp"), rows_dev, shared_out.shape[-1])
    terms_out = pieces.astype(jnp.bfloat16)
    summed = (
        lax.psum_scatter(
            lax.optimization_barrier(terms_out).astype(jnp.float32).astype(jnp.bfloat16),
            "tp",
            scatter_dimension=0,
            tiled=True,
        )
        .astype(jnp.float32)[0]
        .astype(jnp.bfloat16)
    )
    returned = lax.all_to_all(local_routed, "sp", split_axis=0, concat_axis=0, tiled=True)
    picked = (
        returned[targets].reshape(rows_dev, route_count, returned.shape[-1]).astype(jnp.float32)
    )
    routed_sum = jnp.sum(route_weight[:, :, None] * picked, axis=1)
    return (stream_wide + summed.astype(jnp.float32) + routed_sum).astype(jnp.bfloat16)


MESH = pl.DeviceIdType.MESH


def peer_barrier(peers):
    barrier = pltpu.get_barrier_semaphore()
    for peer in peers:
        pl.semaphore_signal(barrier, inc=1, device_id=peer, device_id_type=MESH)
    pl.semaphore_wait(barrier, len(peers))


def remote(src, dst, send_sem, recv_sem, peer):
    return pltpu.make_async_remote_copy(
        src_ref=src,
        dst_ref=dst,
        send_sem=send_sem,
        recv_sem=recv_sem,
        device_id=peer,
        device_id_type=MESH,
    )


def grid_place(sp):
    s = lax.axis_index("sp")
    t = lax.axis_index("tp")
    return s, t, s // 2, s % 2, sp // 2


def gather_kernel(sp, tp, count, with_tp, *refs):
    ins, refs = refs[:count], refs[count:]
    outs, refs = refs[:count], refs[count:]
    if with_tp:
        tp_out, refs = refs[0], refs[1:]
    send_sem, recv_sem, local_sem = refs[:3]
    s, t, z, x, depth = grid_place(sp)
    line = [(lax.rem(z + k, depth) * 2 + x, t) for k in range(1, depth)]
    across = (z * 2 + (1 - x), t)
    columns = [(s, lax.rem(t + k, tp)) for k in range(1, tp)] if with_tp else []
    peer_barrier(line + [across] + columns)
    copies = []
    arrivals = []
    for i in range(count):
        for k in (1, 3, 2) if depth == 4 else range(1, depth):
            copy = remote(
                ins[i], outs[i].at[s], send_sem.at[i, k], recv_sem.at[i, k], line[k - 1]
            )
            copy.start()
            copies.append(copy)
            arrivals.append((k, i, copy))
    for i in range(count):
        copy = remote(
            ins[i], outs[i].at[s], send_sem.at[i, depth], recv_sem.at[i, depth], across
        )
        copy.start()
        copies.append(copy)
    side = []
    if with_tp:
        for k in range(1, tp):
            copy = remote(
                ins[0],
                tp_out.at[t],
                send_sem.at[0, 2 * depth + k],
                recv_sem.at[0, 2 * depth + k],
                columns[k - 1],
            )
            copy.start()
            side.append(copy)
        own = pltpu.make_async_copy(ins[0], tp_out.at[t], local_sem.at[count])
        own.start()
    locals_ = []
    for i in range(count):
        copy = pltpu.make_async_copy(ins[i], outs[i].at[s], local_sem.at[i])
        copy.start()
        locals_.append(copy)
    order = {1: 0, 3: 1, 2: 2}
    arrivals.sort(key=lambda item: (order.get(item[0], item[0]), item[1]))
    for k, i, copy in arrivals:
        copy.wait_recv()
        origin = lax.rem(z + depth - k, depth) * 2 + x
        relay = remote(
            outs[i].at[origin],
            outs[i].at[origin],
            send_sem.at[i, depth + k],
            recv_sem.at[i, depth + k],
            across,
        )
        relay.start()
        side.append(relay)
    for _, _, copy in arrivals:
        copy.wait_send()
    for copy in copies:
        if not any(copy is entry[2] for entry in arrivals):
            copy.wait()
    for copy in side:
        copy.wait()
    for copy in locals_:
        copy.wait()
    if with_tp:
        own.wait()


def gather_sp(arrays, sp, tp, with_tp, collective_id):
    count = len(arrays)
    depth = sp // 2
    shapes = [jax.ShapeDtypeStruct((sp,) + a.shape, a.dtype) for a in arrays]
    if with_tp:
        shapes.append(jax.ShapeDtypeStruct((tp,) + arrays[0].shape, arrays[0].dtype))
    slots = 2 * depth + tp
    return pl.pallas_call(
        partial(gather_kernel, sp, tp, count, with_tp),
        out_shape=tuple(shapes),
        in_specs=[pl.BlockSpec(memory_space=pltpu.VMEM)] * count,
        out_specs=tuple([pl.BlockSpec(memory_space=pltpu.VMEM)] * len(shapes)),
        scratch_shapes=[
            pltpu.SemaphoreType.DMA((count, slots)),
            pltpu.SemaphoreType.DMA((count, slots)),
            pltpu.SemaphoreType.DMA((count + 1,)),
        ],
        compiler_params=pltpu.CompilerParams(
            collective_id=collective_id,
            has_side_effects=True,
            vmem_limit_bytes=16 * 1024 * 1024,
        ),
        cost_estimate=pl.CostEstimate(flops=0, bytes_accessed=40_000_000, transcendentals=0),
    )(*arrays)


def heads_kernel(tp, x_ref, out_ref, send_sem, recv_sem, local_sem):
    s = lax.axis_index("sp")
    t = lax.axis_index("tp")
    width = x_ref.shape[1]
    rows = out_ref.shape[0]
    targets = [lax.rem(t + k, tp) for k in range(1, tp)]
    peer_barrier([(s, target) for target in targets])
    mine = pl.ds(pl.multiple_of(t * width, width), width)
    copies = []
    for k, target in zip(range(1, tp), targets):
        copy = remote(
            x_ref.at[pl.ds(pl.multiple_of(target * rows, rows), rows)],
            out_ref.at[:, mine],
            send_sem.at[k],
            recv_sem.at[k],
            (s, target),
        )
        copy.start()
        copies.append(copy)
    own = pltpu.make_async_copy(
        x_ref.at[pl.ds(pl.multiple_of(t * rows, rows), rows)], out_ref.at[:, mine], local_sem
    )
    own.start()
    for copy in copies:
        copy.wait()
    own.wait()


def exchange_heads(attended, tp, collective_id):
    tokens, width = attended.shape
    return pl.pallas_call(
        partial(heads_kernel, tp),
        out_shape=jax.ShapeDtypeStruct((tokens // tp, tp * width), attended.dtype),
        in_specs=[pl.BlockSpec(memory_space=pltpu.VMEM)],
        out_specs=pl.BlockSpec(memory_space=pltpu.VMEM),
        scratch_shapes=[
            pltpu.SemaphoreType.DMA((tp,)),
            pltpu.SemaphoreType.DMA((tp,)),
            pltpu.SemaphoreType.DMA,
        ],
        compiler_params=pltpu.CompilerParams(
            collective_id=collective_id,
            has_side_effects=True,
            vmem_limit_bytes=16 * 1024 * 1024,
        ),
        cost_estimate=pl.CostEstimate(flops=0, bytes_accessed=5_000_000, transcendentals=0),
    )(attended)


def moe_kernel(sp, *refs):
    normed_ref, stream_ref, weight_ref = refs[:3]
    sources = refs[3:17]
    out_ref = refs[17]
    gate, up, down, sgate, sup, sdown = refs[18:24]
    rows, hid_own, hid_out, hid_in, parts, xin, zout, zin, sout, sin = refs[24:34]
    zs, zr, xs, xr, ys, yr, hs, hr, os_, or_, rs, rr, ss, sr, wsem = refs[34:]
    s, t, z, x, depth = grid_place(sp)
    count, width = normed_ref.shape
    quarter = sources[0].shape[1]
    y, c = t // 2, t % 2
    across = (z * 2 + (1 - x), t)
    mirror = (s, (1 - y) * 2 + c)
    line = [(lax.rem(z + k, depth) * 2 + x, t) for k in range(1, depth)]
    first, second = pl.ds(0, quarter), pl.ds(quarter, quarter)
    places = (
        gate.at[:, first],
        gate.at[:, second],
        up.at[:, first],
        up.at[:, second],
        sgate.at[:, first],
        sgate.at[:, second],
        sup.at[:, first],
        sup.at[:, second],
        sdown.at[first],
        sdown.at[second],
    ) + tuple(down.at[pl.ds(q * quarter, quarter)] for q in range(4))
    loads = [
        pltpu.make_async_copy(source, place, wsem.at[n])
        for n, (source, place) in enumerate(zip(sources, places))
    ]
    for load in loads:
        load.start()
    peer_barrier(line + [across, mirror])

    z_rows, x_rows, y_rows, hids, x_outs, z_outs = {}, {}, {}, {}, {}, {}

    def send_y(j, xx, source):
        y_rows[j, xx] = remote(
            source, rows.at[1, j, xx], ys.at[2 * j + xx], yr.at[2 * j + xx], mirror
        )
        y_rows[j, xx].start()

    def send_x(j, source):
        x_rows[j] = remote(source, rows.at[0, j, 1], xs.at[j], xr.at[j], across)
        x_rows[j].start()

    order = [0, 1, 3, 2] if depth == 4 else list(range(depth))
    send_y(0, 0, normed_ref)
    send_x(0, normed_ref)
    for j in order[1:]:
        k = depth - j
        z_rows[j] = remote(
            normed_ref, rows.at[0, j, 0], zs.at[k - 1], zr.at[k - 1], line[k - 1]
        )
        z_rows[j].start()
    rows[0, 0, 0] = normed_ref[...]

    def hidden_of(block, gate_buf, up_buf):
        gate_value = jnp.dot(block, gate_buf[...], preferred_element_type=jnp.float32)
        up_value = jnp.dot(block, up_buf[...], preferred_element_type=jnp.float32)
        return (jax.nn.silu(gate_value) * up_value).astype(jnp.bfloat16)

    def relay(j):
        if j == 0:
            return
        z_rows[j].wait_recv()
        send_x(j, rows.at[0, j, 0])
        send_y(j, 0, rows.at[0, j, 0])

    def own_plane(j):
        x_rows[j].wait_recv()
        send_y(j, 1, rows.at[0, j, 1])
        if j == 0:
            for load in loads[:4]:
                load.wait()
        hid_own[j] = hidden_of(rows[0, j].reshape(2 * count, width), gate, up)

    def other_plane(j):
        if j != 0:
            y_rows[j, 0].wait_recv()
        y_rows[j, 1].wait_recv()
        hid_out[j] = hidden_of(rows[1, j].reshape(2 * count, width), gate, up)
        hids[j] = remote(hid_out.at[j], hid_in.at[j], hs.at[j], hr.at[j], mirror)
        hids[j].start()

    def finish_down(j):
        if j == 0:
            for load in loads[10:]:
                load.wait()
        hids[j].wait_recv()
        half = hid_own.shape[2]
        value = jnp.dot(
            hid_own[j], down[pl.ds(0, half)], preferred_element_type=jnp.float32
        ) + jnp.dot(hid_in[j], down[pl.ds(half, half)], preferred_element_type=jnp.float32)
        base = lax.rem(z + j, depth) * 2
        parts[j, 1] = (value[count:] * weight_ref[base + 1 - x]).astype(jnp.bfloat16)
        x_outs[j] = remote(parts.at[j, 1], xin.at[j], os_.at[j], or_.at[j], across)
        x_outs[j].start()
        parts[j, 0] = (value[:count] * weight_ref[base + x]).astype(jnp.bfloat16)

    def fold(j):
        x_outs[j].wait_recv()
        if j == 0:
            return
        zout[j - 1] = (parts[j, 0].astype(jnp.float32) + xin[j].astype(jnp.float32)).astype(
            jnp.bfloat16
        )
        z_outs[j] = remote(
            zout.at[j - 1], zin.at[j - 1], rs.at[j - 1], rr.at[j - 1], line[j - 1]
        )
        z_outs[j].start()

    relay(order[1])
    own_plane(order[0])
    y_rows[0, 0].wait_recv()
    for load in loads[4:10]:
        load.wait()
    pair = jnp.concatenate([normed_ref[...], rows[1, 0, 0]], axis=0)
    shared = jnp.dot(
        hidden_of(pair, sgate, sup), sdown[...], preferred_element_type=jnp.float32
    )
    sout[...] = shared[count:].astype(jnp.bfloat16)
    shared_copy = remote(sout, sin, ss, sr, mirror)
    shared_copy.start()
    total = stream_ref[...].astype(jnp.float32) + shared[:count]
    relay(order[2])
    own_plane(order[1])
    other_plane(order[0])
    relay(order[3])
    own_plane(order[2])
    other_plane(order[1])
    finish_down(order[0])
    own_plane(order[3])
    other_plane(order[2])
    finish_down(order[1])
    fold(order[0])
    other_plane(order[3])
    finish_down(order[2])
    fold(order[1])
    finish_down(order[3])
    fold(order[2])
    fold(order[3])
    shared_copy.wait_recv()
    total = total + sin[...].astype(jnp.float32)
    total = total + parts[0, 0].astype(jnp.float32) + xin[0].astype(jnp.float32)
    for j in order[1:]:
        z_outs[j].wait_recv()
        total = total + zin[j - 1].astype(jnp.float32)
    out_ref[...] = total.astype(out_ref.dtype)
    for group in (z_rows, x_rows, y_rows, hids, x_outs, z_outs):
        for copy in group.values():
            copy.wait_send()
    shared_copy.wait_send()


def run_moe(normed, stream, weights, sources, sp, collective_id):
    count, width = normed.shape
    depth = sp // 2
    quarter = sources[0].shape[1]
    half = 2 * quarter
    vmem = pl.BlockSpec(memory_space=pltpu.VMEM)

    def dma(n):
        return [pltpu.SemaphoreType.DMA((n,))] * 2

    bf16 = jnp.bfloat16
    return pl.pallas_call(
        partial(moe_kernel, sp),
        out_shape=jax.ShapeDtypeStruct((count, width), bf16),
        in_specs=[vmem] * 3 + [pl.BlockSpec(memory_space=pl.ANY)] * len(sources),
        out_specs=vmem,
        scratch_shapes=[
            pltpu.VMEM((width, half), bf16),
            pltpu.VMEM((width, half), bf16),
            pltpu.VMEM((2 * half, width), bf16),
            pltpu.VMEM((width, half), bf16),
            pltpu.VMEM((width, half), bf16),
            pltpu.VMEM((half, width), bf16),
            pltpu.VMEM((2, depth, 2, count, width), bf16),
            pltpu.VMEM((depth, 2 * count, half), bf16),
            pltpu.VMEM((depth, 2 * count, half), bf16),
            pltpu.VMEM((depth, 2 * count, half), bf16),
            pltpu.VMEM((depth, 2, count, width), bf16),
            pltpu.VMEM((depth, count, width), bf16),
            pltpu.VMEM((depth - 1, count, width), bf16),
            pltpu.VMEM((depth - 1, count, width), bf16),
            pltpu.VMEM((count, width), bf16),
            pltpu.VMEM((count, width), bf16),
        ]
        + dma(depth - 1)
        + dma(depth)
        + dma(2 * depth)
        + dma(depth)
        + dma(depth)
        + dma(depth - 1)
        + [pltpu.SemaphoreType.DMA] * 2
        + [pltpu.SemaphoreType.DMA((len(sources),))],
        compiler_params=pltpu.CompilerParams(
            collective_id=collective_id,
            has_side_effects=True,
            vmem_limit_bytes=44 * 1024 * 1024,
        ),
        cost_estimate=pl.CostEstimate(
            flops=12 * depth * count * width * half * 3,
            bytes_accessed=30_000_000,
            transcendentals=0,
        ),
    )(normed, stream, weights, *sources)


def dense_body(
    query_maps,
    key_maps,
    value_rows,
    mix_lambda,
    head_gain,
    out_weight,
    residual,
    norm_gain,
    routes,
    route_weight,
    expert_gate,
    expert_up,
    expert_down,
    shared_gate,
    shared_up,
    shared_down,
):
    sp = lax.axis_size("sp")
    tp = lax.axis_size("tp")
    s = lax.axis_index("sp")
    t = lax.axis_index("tp")

    def swapped(array, step):
        return lax.ppermute(array, "tp", [(i, i ^ step) for i in range(tp)])

    own_gate, own_up, own_down = expert_gate[0], expert_up[0], expert_down[0]
    far_down = swapped(own_down, 2)
    near_gate = swapped(own_gate, 1)
    near_up = swapped(own_up, 1)
    near_sgate = swapped(shared_gate, 1)
    near_sup = swapped(shared_up, 1)
    near_sdown = swapped(shared_down, 1)
    near_down = swapped(own_down, 1)

    local_heads = mix_lambda.shape[0]
    head_width = head_gain.shape[0]
    kv_local = value_rows.shape[1] // head_width
    head_group = local_heads // kv_local
    head_dim = key_maps.shape[1] // (2 * kv_local)
    token_count = query_maps.shape[0]
    rows_dev = token_count // tp
    experts = sp

    own_routes = lax.dynamic_slice_in_dim(routes, t * rows_dev, rows_dev, 0)
    named = own_routes[None, :, :] == jnp.arange(experts, dtype=jnp.int32)[:, None, None]
    table = jnp.sum(jnp.where(named, route_weight[None], 0.0), axis=2)
    lanes = -(-rows_dev // 128) * 128
    table = jnp.pad(table, ((0, 0), (0, lanes - rows_dev)))

    key_all, value_all, tables = gather_sp([key_maps, value_rows, table], sp, tp, False, 1)
    key_all = key_all.reshape(sp * token_count, -1)
    value_all = value_all.reshape(sp * token_count, -1)
    weights = lax.dynamic_index_in_dim(tables, s, 1, False)[:, :rows_dev, None]

    queries = query_maps.reshape(token_count, kv_local, head_group, 2, head_dim)
    start_max = jnp.full((kv_local, head_group, 2, token_count), lowest_score, jnp.float32)
    start_sum = jnp.zeros((kv_local, head_group, 2, token_count), jnp.float32)
    start_values = jnp.zeros((kv_local, head_group, 2, token_count, head_width), jnp.float32)
    _, run_sum, accumulated = fold_keys(
        (start_max, start_sum, start_values),
        (key_all, value_all),
        jnp.int32(0),
        queries,
        head_dim ** (-0.5),
    )
    normalized = accumulated / run_sum[..., None]
    lambdas = mix_lambda.reshape(kv_local, head_group, 1, 1)
    difference = normalized[:, :, 0] - lambdas * normalized[:, :, 1]
    inverse_rms = lax.rsqrt(jnp.mean(difference * difference, axis=-1, keepdims=True) + norm_eps)
    head_scaled = (difference * inverse_rms * head_gain).astype(jnp.bfloat16)
    attended = jnp.transpose(head_scaled, (2, 0, 1, 3)).reshape(
        token_count, local_heads * head_width
    )
    attended = exchange_heads(attended, tp, 2)
    projected = jnp.dot(attended, out_weight, preferred_element_type=jnp.float32)
    stream = (residual.astype(jnp.float32) + projected).astype(jnp.bfloat16)
    stream_wide = stream.astype(jnp.float32)
    stream_rms = lax.rsqrt(jnp.mean(stream_wide * stream_wide, axis=1, keepdims=True) + norm_eps)
    normed = (stream_wide * stream_rms * norm_gain).astype(jnp.bfloat16)
    far_near_down = swapped(far_down, 1)
    return run_moe(
        normed,
        stream,
        weights,
        (
            own_gate,
            near_gate,
            own_up,
            near_up,
            shared_gate,
            near_sgate,
            shared_up,
            near_sup,
            shared_down,
            near_sdown,
            own_down,
            near_down,
            far_down,
            far_near_down,
        ),
        sp,
        4,
    )


def solution(mesh):
    in_specs = (
        P("sp", "tp"),
        P("sp", "tp"),
        P("sp", "tp"),
        P("tp"),
        P(),
        P(),
        P(("sp", "tp"), None),
        P(),
        P("sp", None),
        P(("sp", "tp"), None),
        P("sp", None, "tp"),
        P("sp", None, "tp"),
        P("sp", "tp", None),
        P(None, "tp"),
        P(None, "tp"),
        P("tp", None),
    )
    out_specs = P(("sp", "tp"), None)
    sp, tp = mesh.shape["sp"], mesh.shape["tp"]

    def chosen(*args):
        route_count = args[8].shape[1]
        experts = sp * args[10].shape[0]
        rows_dev = args[6].shape[0]
        whole_blocks = 2 * rows_dev * route_count >= experts * rows_dev
        dense = whole_blocks and args[10].shape[0] == 1 and sp == 8 and tp == 4
        if not dense:
            return body(*args)
        return dense_body(*args)

    return jax.shard_map(
        chosen, mesh=mesh, in_specs=in_specs, out_specs=out_specs, check_vma=False
    )
```

```python
from functools import partial

import jax
import jax.numpy as jnp
from jax import lax
from jax.experimental import pallas as pl
from jax.experimental.pallas import tpu as pltpu
from jax.sharding import PartitionSpec as P


norm_eps = 1e-06
lowest_score = -1e30


def slot_targets(block_routes, experts, capacity):
    flat_routes = block_routes.reshape(-1)
    onehot = (flat_routes[:, None] == jnp.arange(experts, dtype=jnp.int32)[None, :]).astype(
        jnp.int32
    )
    earlier = jnp.cumsum(onehot, axis=0) - onehot
    return flat_routes * capacity + jnp.sum(earlier * onehot, axis=1)


def build_buffer(token_rows, block_routes, experts, capacity):
    targets = slot_targets(block_routes, experts, capacity)
    row_total = block_routes.shape[0]
    route_count = block_routes.shape[1]
    source_row = jnp.arange(row_total * route_count, dtype=jnp.int32) // route_count
    holder = jnp.full((experts * capacity,), row_total, jnp.int32).at[targets].set(source_row)
    padded = jnp.concatenate(
        [token_rows, jnp.zeros((1, token_rows.shape[1]), token_rows.dtype)], axis=0
    )
    return (padded[holder], targets)


def attention_block(carried, queries, key_block, value_block, score_scale):
    run_max, run_sum, accumulated = carried
    kv_local = run_max.shape[0]
    key_heads = key_block.reshape(key_block.shape[0], kv_local, 2, -1)
    value_heads = value_block.reshape(value_block.shape[0], kv_local, -1)
    scores = (
        jnp.einsum("qagcd,racd->agcqr", queries, key_heads, preferred_element_type=jnp.float32)
        * score_scale
    )
    new_max = jnp.maximum(run_max, jnp.max(scores, axis=-1))
    rescale = jnp.exp(run_max - new_max)
    weights = jnp.exp(scores - new_max[..., None])
    run_sum = run_sum * rescale + jnp.sum(weights, axis=-1)
    update = jnp.einsum(
        "agcqr,rae->agcqe",
        weights.astype(jnp.bfloat16),
        value_heads,
        preferred_element_type=jnp.float32,
    )
    return (new_max, run_sum, accumulated * rescale[..., None] + update)


def fold_keys(carried, pieces, first_row, queries, score_scale):
    key_piece, value_piece = pieces
    total_rows = key_piece.shape[0]
    block_rows = total_rows
    for candidate in (2048, 1024, 512):
        if total_rows % candidate == 0:
            block_rows = candidate
            break
    block_count = total_rows // block_rows

    def block_step(block_index, running):
        start_row = block_index * block_rows
        return attention_block(
            running,
            queries,
            lax.dynamic_slice_in_dim(key_piece, start_row, block_rows, 0),
            lax.dynamic_slice_in_dim(value_piece, start_row, block_rows, 0),
            score_scale,
        )

    return lax.fori_loop(0, block_count, block_step, carried)


def whole_experts(arrived, whole_gate, whole_up, whole_down, senders, capacity, groups):
    local_experts = whole_gate.shape[0]
    width = arrived.shape[-1]
    rows_in = arrived.reshape(senders, local_experts, capacity, width)
    gate_value = jnp.einsum(
        "sjtd,jdf->sjtf", rows_in, whole_gate, preferred_element_type=jnp.float32
    )
    up_value = jnp.einsum("sjtd,jdf->sjtf", rows_in, whole_up, preferred_element_type=jnp.float32)
    hidden = (jax.nn.silu(gate_value) * up_value).astype(jnp.bfloat16)
    hidden_units = hidden.shape[-1]
    hidden = hidden.reshape(senders, local_experts, capacity, groups, hidden_units // groups)
    down_groups = whole_down.reshape(local_experts, groups, hidden_units // groups, width)
    group_sums = jnp.einsum(
        "sjtgf,jgfd->sjtgd", hidden, down_groups, preferred_element_type=jnp.float32
    )
    group_sums = lax.optimization_barrier(group_sums.astype(jnp.bfloat16)).astype(jnp.float32)
    return (
        jnp.sum(group_sums, axis=3)
        .astype(jnp.bfloat16)
        .reshape(senders * local_experts * capacity, width)
    )


def body(
    query_maps,
    key_maps,
    value_rows,
    mix_lambda,
    head_gain,
    out_weight,
    residual,
    norm_gain,
    routes,
    route_weight,
    expert_gate,
    expert_up,
    expert_down,
    shared_gate,
    shared_up,
    shared_down,
):
    local_heads = mix_lambda.shape[0]
    head_width = head_gain.shape[0]
    kv_local = value_rows.shape[1] // head_width
    head_group = local_heads // kv_local
    head_dim = key_maps.shape[1] // (2 * kv_local)
    token_count = query_maps.shape[0]
    queries = query_maps.reshape(token_count, kv_local, head_group, 2, head_dim)
    start_max = jnp.full((kv_local, head_group, 2, token_count), lowest_score, jnp.float32)
    start_sum = jnp.zeros((kv_local, head_group, 2, token_count), jnp.float32)
    start_values = jnp.zeros((kv_local, head_group, 2, token_count, head_width), jnp.float32)
    folder = partial(fold_keys, queries=queries, score_scale=head_dim ** (-0.5))
    _, run_sum, accumulated = folder(
        (start_max, start_sum, start_values),
        (
            lax.all_gather(key_maps, "sp", axis=0, tiled=True),
            lax.all_gather(value_rows, "sp", axis=0, tiled=True),
        ),
        jnp.int32(0),
    )
    normalized = accumulated / run_sum[..., None]
    lambdas = mix_lambda.reshape(kv_local, head_group, 1, 1)
    difference = normalized[:, :, 0] - lambdas * normalized[:, :, 1]
    inverse_rms = lax.rsqrt(jnp.mean(difference * difference, axis=-1, keepdims=True) + norm_eps)
    head_scaled = (difference * inverse_rms * head_gain).astype(jnp.bfloat16)
    attended = jnp.transpose(head_scaled, (2, 0, 1, 3)).reshape(
        token_count, local_heads * head_width
    )
    columns = lax.axis_size("tp")
    column = lax.axis_index("tp")
    rows_dev = token_count // columns
    own_rows = lax.dynamic_slice_in_dim(
        out_weight, column * attended.shape[1], attended.shape[1], 0
    )
    projected = lax.psum_scatter(
        jnp.dot(attended, own_rows, preferred_element_type=jnp.float32).astype(jnp.bfloat16),
        "tp",
        scatter_dimension=0,
        tiled=True,
    ).astype(jnp.float32)
    stream = (residual.astype(jnp.float32) + projected).astype(jnp.bfloat16)
    stream_wide = stream.astype(jnp.float32)
    stream_rms = lax.rsqrt(jnp.mean(stream_wide * stream_wide, axis=1, keepdims=True) + norm_eps)
    normed = (stream_wide * stream_rms * norm_gain).astype(jnp.bfloat16)
    senders = lax.axis_size("sp")
    local_experts = expert_gate.shape[0]
    experts = senders * local_experts
    route_count = routes.shape[1]
    capacity = max(2, 2 * rows_dev * route_count // experts)
    local_routed = None
    whole_gate, whole_up, whole_down = (
        lax.all_gather(expert_gate, "tp", axis=2, tiled=True),
        lax.all_gather(expert_up, "tp", axis=2, tiled=True),
        lax.all_gather(expert_down, "tp", axis=1, tiled=True),
    )
    own_routes = lax.dynamic_slice_in_dim(routes, column * rows_dev, rows_dev, 0)
    buffer, targets = build_buffer(normed, own_routes, experts, capacity)
    arrived = lax.all_to_all(buffer, "sp", split_axis=0, concat_axis=0, tiled=True)
    local_routed = whole_experts(
        arrived, whole_gate, whole_up, whole_down, senders, capacity, columns
    )
    shared_rows = lax.all_gather(normed[None], "tp", axis=0, tiled=True)
    shared_in = shared_rows
    shared_in = shared_in.reshape(1 * lax.axis_size("tp") * rows_dev, shared_in.shape[-1])
    shared_hidden = (
        jax.nn.silu(jnp.dot(shared_in, shared_gate, preferred_element_type=jnp.float32))
        * jnp.dot(shared_in, shared_up, preferred_element_type=jnp.float32)
    ).astype(jnp.bfloat16)
    shared_out = jnp.dot(shared_hidden, shared_down, preferred_element_type=jnp.float32)
    pieces = shared_out.reshape(1 * lax.axis_size("tp"), rows_dev, shared_out.shape[-1])
    terms_out = pieces.astype(jnp.bfloat16)
    summed = (
        lax.psum_scatter(
            lax.optimization_barrier(terms_out).astype(jnp.float32).astype(jnp.bfloat16),
            "tp",
            scatter_dimension=0,
            tiled=True,
        )
        .astype(jnp.float32)[0]
        .astype(jnp.bfloat16)
    )
    returned = lax.all_to_all(local_routed, "sp", split_axis=0, concat_axis=0, tiled=True)
    picked = (
        returned[targets].reshape(rows_dev, route_count, returned.shape[-1]).astype(jnp.float32)
    )
    routed_sum = jnp.sum(route_weight[:, :, None] * picked, axis=1)
    return (stream_wide + summed.astype(jnp.float32) + routed_sum).astype(jnp.bfloat16)


MESH = pl.DeviceIdType.MESH


def peer_barrier(peers):
    barrier = pltpu.get_barrier_semaphore()
    for peer in peers:
        pl.semaphore_signal(barrier, inc=1, device_id=peer, device_id_type=MESH)
    pl.semaphore_wait(barrier, len(peers))


def remote(src, dst, send_sem, recv_sem, peer):
    return pltpu.make_async_remote_copy(
        src_ref=src,
        dst_ref=dst,
        send_sem=send_sem,
        recv_sem=recv_sem,
        device_id=peer,
        device_id_type=MESH,
    )


def grid_place(sp):
    s = lax.axis_index("sp")
    t = lax.axis_index("tp")
    return s, t, s // 2, s % 2, sp // 2


def gather_kernel(sp, tp, count, with_tp, *refs):
    ins, refs = refs[:count], refs[count:]
    outs, refs = refs[:count], refs[count:]
    if with_tp:
        tp_out, refs = refs[0], refs[1:]
    send_sem, recv_sem, local_sem = refs[:3]
    s, t, z, x, depth = grid_place(sp)
    line = [(lax.rem(z + k, depth) * 2 + x, t) for k in range(1, depth)]
    across = (z * 2 + (1 - x), t)
    columns = [(s, lax.rem(t + k, tp)) for k in range(1, tp)] if with_tp else []
    peer_barrier(line + [across] + columns)
    copies = []
    arrivals = []
    for i in range(count):
        for k in (1, 3, 2) if depth == 4 else range(1, depth):
            copy = remote(
                ins[i], outs[i].at[s], send_sem.at[i, k], recv_sem.at[i, k], line[k - 1]
            )
            copy.start()
            copies.append(copy)
            arrivals.append((k, i, copy))
    for i in range(count):
        copy = remote(
            ins[i], outs[i].at[s], send_sem.at[i, depth], recv_sem.at[i, depth], across
        )
        copy.start()
        copies.append(copy)
    side = []
    if with_tp:
        for k in range(1, tp):
            copy = remote(
                ins[0],
                tp_out.at[t],
                send_sem.at[0, 2 * depth + k],
                recv_sem.at[0, 2 * depth + k],
                columns[k - 1],
            )
            copy.start()
            side.append(copy)
        own = pltpu.make_async_copy(ins[0], tp_out.at[t], local_sem.at[count])
        own.start()
    locals_ = []
    for i in range(count):
        copy = pltpu.make_async_copy(ins[i], outs[i].at[s], local_sem.at[i])
        copy.start()
        locals_.append(copy)
    order = {1: 0, 3: 1, 2: 2}
    arrivals.sort(key=lambda item: (order.get(item[0], item[0]), item[1]))
    for k, i, copy in arrivals:
        copy.wait_recv()
        origin = lax.rem(z + depth - k, depth) * 2 + x
        relay = remote(
            outs[i].at[origin],
            outs[i].at[origin],
            send_sem.at[i, depth + k],
            recv_sem.at[i, depth + k],
            across,
        )
        relay.start()
        side.append(relay)
    for _, _, copy in arrivals:
        copy.wait_send()
    for copy in copies:
        if not any(copy is entry[2] for entry in arrivals):
            copy.wait()
    for copy in side:
        copy.wait()
    for copy in locals_:
        copy.wait()
    if with_tp:
        own.wait()


def gather_sp(arrays, sp, tp, with_tp, collective_id):
    count = len(arrays)
    depth = sp // 2
    shapes = [jax.ShapeDtypeStruct((sp,) + a.shape, a.dtype) for a in arrays]
    if with_tp:
        shapes.append(jax.ShapeDtypeStruct((tp,) + arrays[0].shape, arrays[0].dtype))
    slots = 2 * depth + tp
    return pl.pallas_call(
        partial(gather_kernel, sp, tp, count, with_tp),
        out_shape=tuple(shapes),
        in_specs=[pl.BlockSpec(memory_space=pltpu.VMEM)] * count,
        out_specs=tuple([pl.BlockSpec(memory_space=pltpu.VMEM)] * len(shapes)),
        scratch_shapes=[
            pltpu.SemaphoreType.DMA((count, slots)),
            pltpu.SemaphoreType.DMA((count, slots)),
            pltpu.SemaphoreType.DMA((count + 1,)),
        ],
        compiler_params=pltpu.CompilerParams(
            collective_id=collective_id,
            has_side_effects=True,
            vmem_limit_bytes=16 * 1024 * 1024,
        ),
        cost_estimate=pl.CostEstimate(flops=0, bytes_accessed=40_000_000, transcendentals=0),
    )(*arrays)


def heads_kernel(tp, x_ref, out_ref, send_sem, recv_sem, local_sem):
    s = lax.axis_index("sp")
    t = lax.axis_index("tp")
    width = x_ref.shape[1]
    rows = out_ref.shape[0]
    targets = [lax.rem(t + k, tp) for k in range(1, tp)]
    peer_barrier([(s, target) for target in targets])
    mine = pl.ds(pl.multiple_of(t * width, width), width)
    copies = []
    for k, target in zip(range(1, tp), targets):
        copy = remote(
            x_ref.at[pl.ds(pl.multiple_of(target * rows, rows), rows)],
            out_ref.at[:, mine],
            send_sem.at[k],
            recv_sem.at[k],
            (s, target),
        )
        copy.start()
        copies.append(copy)
    own = pltpu.make_async_copy(
        x_ref.at[pl.ds(pl.multiple_of(t * rows, rows), rows)], out_ref.at[:, mine], local_sem
    )
    own.start()
    for copy in copies:
        copy.wait()
    own.wait()


def exchange_heads(attended, tp, collective_id):
    tokens, width = attended.shape
    return pl.pallas_call(
        partial(heads_kernel, tp),
        out_shape=jax.ShapeDtypeStruct((tokens // tp, tp * width), attended.dtype),
        in_specs=[pl.BlockSpec(memory_space=pltpu.VMEM)],
        out_specs=pl.BlockSpec(memory_space=pltpu.VMEM),
        scratch_shapes=[
            pltpu.SemaphoreType.DMA((tp,)),
            pltpu.SemaphoreType.DMA((tp,)),
            pltpu.SemaphoreType.DMA,
        ],
        compiler_params=pltpu.CompilerParams(
            collective_id=collective_id,
            has_side_effects=True,
            vmem_limit_bytes=16 * 1024 * 1024,
        ),
        cost_estimate=pl.CostEstimate(flops=0, bytes_accessed=5_000_000, transcendentals=0),
    )(attended)


def moe_kernel(sp, *refs):
    normed_ref, stream_ref, weight_ref = refs[:3]
    sources = refs[3:17]
    out_ref = refs[17]
    gate, up, down, sgate, sup, sdown = refs[18:24]
    rows, hid_own, hid_out, hid_in, parts, xin, zout, zin, sout, sin, total = refs[24:35]
    zs, zr, xs, xr, ys, yr, hs, hr, os_, or_, rs, rr, ss, sr, wsem = refs[35:]
    s, t, z, x, depth = grid_place(sp)
    count, width = normed_ref.shape
    quarter = sources[0].shape[1]
    y, c = t // 2, t % 2
    across = (z * 2 + (1 - x), t)
    mirror = (s, (1 - y) * 2 + c)
    line = [(lax.rem(z + k, depth) * 2 + x, t) for k in range(1, depth)]
    first, second = pl.ds(0, quarter), pl.ds(quarter, quarter)
    places = (
        gate.at[:, first],
        gate.at[:, second],
        up.at[:, first],
        up.at[:, second],
        sgate.at[:, first],
        sgate.at[:, second],
        sup.at[:, first],
        sup.at[:, second],
        sdown.at[first],
        sdown.at[second],
    ) + tuple(down.at[pl.ds(q * quarter, quarter)] for q in range(4))
    loads = [
        pltpu.make_async_copy(source, place, wsem.at[n])
        for n, (source, place) in enumerate(zip(sources, places))
    ]
    for load in loads:
        load.start()
    peer_barrier(line + [across, mirror])

    z_rows, started = {}, []
    x_rows, y_rows, diagonal, hids, x_outs, z_outs = {}, {}, {}, {}, {}, {}

    def send(source, target, send_sem, recv_sem, peer):
        copy = remote(source, target, send_sem, recv_sem, peer)
        copy.start()
        started.append(copy)
        return copy

    def own_rows(j):
        return normed_ref if j == 0 else rows.at[0, j, 0]

    def hidden_of(block, gate_buf, up_buf):
        gate_value = jnp.dot(block, gate_buf[...], preferred_element_type=jnp.float32)
        up_value = jnp.dot(block, up_buf[...], preferred_element_type=jnp.float32)
        return (jax.nn.silu(gate_value) * up_value).astype(jnp.bfloat16)

    waited = set()

    def arrived(copies, j):
        if (id(copies), j) not in waited:
            waited.add((id(copies), j))
            copies[j].wait_recv()

    def loaded(first_load, last_load):
        for n in range(first_load, last_load):
            if ("load", n) not in waited:
                waited.add(("load", n))
                loads[n].wait()

    def RX(j):
        if j != 0:
            arrived(z_rows, j)
        x_rows[j] = send(own_rows(j), rows.at[0, j, 1], xs.at[j], xr.at[j], across)

    def RY(j):
        if j != 0:
            arrived(z_rows, j)
        y_rows[j] = send(own_rows(j), rows.at[1, j, 0], ys.at[j], yr.at[j], mirror)

    def RD(j):
        sems = ys.at[depth + j], yr.at[depth + j]
        if j in by_x:
            arrived(y_rows, j)
            diagonal[j] = send(rows.at[1, j, 0], rows.at[1, j, 1], *sems, across)
        else:
            arrived(x_rows, j)
            diagonal[j] = send(rows.at[0, j, 1], rows.at[1, j, 1], *sems, mirror)

    def HO(j):
        arrived(x_rows, j)
        loaded(0, 4)
        hid_own[j] = hidden_of(rows[0, j].reshape(2 * count, width), gate, up)

    def HP(j):
        arrived(y_rows, j)
        arrived(diagonal, j)
        loaded(0, 4)
        hid_out[j] = hidden_of(rows[1, j].reshape(2 * count, width), gate, up)
        hids[j] = send(hid_out.at[j], hid_in.at[j], hs.at[j], hr.at[j], mirror)

    def FD(j):
        loaded(10, 14)
        arrived(hids, j)
        half = hid_own.shape[2]
        value = jnp.dot(
            hid_own[j], down[pl.ds(0, half)], preferred_element_type=jnp.float32
        ) + jnp.dot(hid_in[j], down[pl.ds(half, half)], preferred_element_type=jnp.float32)
        base = lax.rem(z + j, depth) * 2
        parts[j, 1] = (value[count:] * weight_ref[base + 1 - x]).astype(jnp.bfloat16)
        x_outs[j] = send(parts.at[j, 1], xin.at[j], os_.at[j], or_.at[j], across)
        parts[j, 0] = (value[:count] * weight_ref[base + x]).astype(jnp.bfloat16)

    def FO(j):
        arrived(x_outs, j)
        zout[j - 1] = (parts[j, 0].astype(jnp.float32) + xin[j].astype(jnp.float32)).astype(
            jnp.bfloat16
        )
        z_outs[j] = send(
            zout.at[j - 1], zin.at[j - 1], rs.at[j - 1], rr.at[j - 1], line[j - 1]
        )

    shared_copy = []

    def SH(j):
        arrived(y_rows, 0)
        loaded(4, 10)
        pair = jnp.concatenate([normed_ref[...], rows[1, 0, 0]], axis=0)
        shared = jnp.dot(
            hidden_of(pair, sgate, sup), sdown[...], preferred_element_type=jnp.float32
        )
        sout[...] = shared[count:].astype(jnp.bfloat16)
        total[...] = stream_ref[...].astype(jnp.float32) + shared[:count]

    def SS(j):
        shared_copy.append(send(sout, sin, ss, sr, mirror))

    actions = {f.__name__: f for f in (RX, RY, RD, HO, HP, FD, FO, SH, SS)}
    by_x, steps = moe_plan()
    rows[0, 0, 0] = normed_ref[...]
    for j in [1, 3, 2] if depth == 4 else range(1, depth):
        k = depth - j
        z_rows[j] = send(
            normed_ref, rows.at[0, j, 0], zs.at[k - 1], zr.at[k - 1], line[k - 1]
        )
    for step in steps:
        actions[step[:2]](int(step[2:] or 0))
    shared_copy[0].wait_recv()
    arrived(x_outs, 0)
    value = total[...] + sin[...].astype(jnp.float32)
    value = value + parts[0, 0].astype(jnp.float32) + xin[0].astype(jnp.float32)
    for j in range(1, depth):
        arrived(z_outs, j)
        value = value + zin[j - 1].astype(jnp.float32)
    out_ref[...] = value.astype(out_ref.dtype)
    for copy in started:
        copy.wait_send()


def moe_plan():
    return (0, 3), [
        step
        for group in (
            "RY0 RX0 RY1 RX1",
            "RY3 RX3 HO1 RD1",
            "RX2 RY2 RD3 HP1",
            "RD0 RD2 HO3 HP3",
            "FD1 HP2 FD3 FO1",
            "HP0 HO2 FD2 FO3",
            "HO0 FD0 FO2 SH",
            "SS",
        )
        for step in group.split()
    ]


def run_moe(normed, stream, weights, sources, sp, collective_id):
    count, width = normed.shape
    depth = sp // 2
    quarter = sources[0].shape[1]
    half = 2 * quarter
    vmem = pl.BlockSpec(memory_space=pltpu.VMEM)

    def dma(n):
        return [pltpu.SemaphoreType.DMA((n,))] * 2

    bf16 = jnp.bfloat16
    return pl.pallas_call(
        partial(moe_kernel, sp),
        out_shape=jax.ShapeDtypeStruct((count, width), bf16),
        in_specs=[vmem] * 3 + [pl.BlockSpec(memory_space=pl.ANY)] * len(sources),
        out_specs=vmem,
        scratch_shapes=[
            pltpu.VMEM((width, half), bf16),
            pltpu.VMEM((width, half), bf16),
            pltpu.VMEM((2 * half, width), bf16),
            pltpu.VMEM((width, half), bf16),
            pltpu.VMEM((width, half), bf16),
            pltpu.VMEM((half, width), bf16),
            pltpu.VMEM((2, depth, 2, count, width), bf16),
            pltpu.VMEM((depth, 2 * count, half), bf16),
            pltpu.VMEM((depth, 2 * count, half), bf16),
            pltpu.VMEM((depth, 2 * count, half), bf16),
            pltpu.VMEM((depth, 2, count, width), bf16),
            pltpu.VMEM((depth, count, width), bf16),
            pltpu.VMEM((depth - 1, count, width), bf16),
            pltpu.VMEM((depth - 1, count, width), bf16),
            pltpu.VMEM((count, width), bf16),
            pltpu.VMEM((count, width), bf16),
            pltpu.VMEM((count, width), jnp.float32),
        ]
        + dma(depth - 1)
        + dma(depth)
        + dma(2 * depth)
        + dma(depth)
        + dma(depth)
        + dma(depth - 1)
        + [pltpu.SemaphoreType.DMA] * 2
        + [pltpu.SemaphoreType.DMA((len(sources),))],
        compiler_params=pltpu.CompilerParams(
            collective_id=collective_id,
            has_side_effects=True,
            vmem_limit_bytes=44 * 1024 * 1024,
        ),
        cost_estimate=pl.CostEstimate(
            flops=12 * depth * count * width * half * 3,
            bytes_accessed=30_000_000,
            transcendentals=0,
        ),
    )(normed, stream, weights, *sources)


def dense_body(
    query_maps,
    key_maps,
    value_rows,
    mix_lambda,
    head_gain,
    out_weight,
    residual,
    norm_gain,
    routes,
    route_weight,
    expert_gate,
    expert_up,
    expert_down,
    shared_gate,
    shared_up,
    shared_down,
):
    sp = lax.axis_size("sp")
    tp = lax.axis_size("tp")
    s = lax.axis_index("sp")
    t = lax.axis_index("tp")

    def swapped(array, step):
        return lax.ppermute(array, "tp", [(i, i ^ step) for i in range(tp)])

    own_gate, own_up, own_down = expert_gate[0], expert_up[0], expert_down[0]
    far_down = swapped(own_down, 2)
    near_gate = swapped(own_gate, 1)
    near_up = swapped(own_up, 1)
    near_sgate = swapped(shared_gate, 1)
    near_sup = swapped(shared_up, 1)
    near_sdown = swapped(shared_down, 1)
    near_down = swapped(own_down, 1)

    local_heads = mix_lambda.shape[0]
    head_width = head_gain.shape[0]
    kv_local = value_rows.shape[1] // head_width
    head_group = local_heads // kv_local
    head_dim = key_maps.shape[1] // (2 * kv_local)
    token_count = query_maps.shape[0]
    rows_dev = token_count // tp
    experts = sp

    own_routes = lax.dynamic_slice_in_dim(routes, t * rows_dev, rows_dev, 0)
    named = own_routes[None, :, :] == jnp.arange(experts, dtype=jnp.int32)[:, None, None]
    table = jnp.sum(jnp.where(named, route_weight[None], 0.0), axis=2)
    lanes = -(-rows_dev // 128) * 128
    table = jnp.pad(table, ((0, 0), (0, lanes - rows_dev)))

    key_all, value_all, tables = gather_sp([key_maps, value_rows, table], sp, tp, False, 1)
    key_all = key_all.reshape(sp * token_count, -1)
    value_all = value_all.reshape(sp * token_count, -1)
    weights = lax.dynamic_index_in_dim(tables, s, 1, False)[:, :rows_dev, None]

    queries = query_maps.reshape(token_count, kv_local, head_group, 2, head_dim)
    start_max = jnp.full((kv_local, head_group, 2, token_count), lowest_score, jnp.float32)
    start_sum = jnp.zeros((kv_local, head_group, 2, token_count), jnp.float32)
    start_values = jnp.zeros((kv_local, head_group, 2, token_count, head_width), jnp.float32)
    _, run_sum, accumulated = fold_keys(
        (start_max, start_sum, start_values),
        (key_all, value_all),
        jnp.int32(0),
        queries,
        head_dim ** (-0.5),
    )
    normalized = accumulated / run_sum[..., None]
    lambdas = mix_lambda.reshape(kv_local, head_group, 1, 1)
    difference = normalized[:, :, 0] - lambdas * normalized[:, :, 1]
    inverse_rms = lax.rsqrt(jnp.mean(difference * difference, axis=-1, keepdims=True) + norm_eps)
    head_scaled = (difference * inverse_rms * head_gain).astype(jnp.bfloat16)
    attended = jnp.transpose(head_scaled, (2, 0, 1, 3)).reshape(
        token_count, local_heads * head_width
    )
    attended = exchange_heads(attended, tp, 2)
    projected = jnp.dot(attended, out_weight, preferred_element_type=jnp.float32)
    stream = (residual.astype(jnp.float32) + projected).astype(jnp.bfloat16)
    stream_wide = stream.astype(jnp.float32)
    stream_rms = lax.rsqrt(jnp.mean(stream_wide * stream_wide, axis=1, keepdims=True) + norm_eps)
    normed = (stream_wide * stream_rms * norm_gain).astype(jnp.bfloat16)
    far_near_down = swapped(far_down, 1)
    return run_moe(
        normed,
        stream,
        weights,
        (
            own_gate,
            near_gate,
            own_up,
            near_up,
            shared_gate,
            near_sgate,
            shared_up,
            near_sup,
            shared_down,
            near_sdown,
            own_down,
            near_down,
            far_down,
            far_near_down,
        ),
        sp,
        4,
    )


def solution(mesh):
    in_specs = (
        P("sp", "tp"),
        P("sp", "tp"),
        P("sp", "tp"),
        P("tp"),
        P(),
        P(),
        P(("sp", "tp"), None),
        P(),
        P("sp", None),
        P(("sp", "tp"), None),
        P("sp", None, "tp"),
        P("sp", None, "tp"),
        P("sp", "tp", None),
        P(None, "tp"),
        P(None, "tp"),
        P("tp", None),
    )
    out_specs = P(("sp", "tp"), None)
    sp, tp = mesh.shape["sp"], mesh.shape["tp"]

    def chosen(*args):
        route_count = args[8].shape[1]
        experts = sp * args[10].shape[0]
        rows_dev = args[6].shape[0]
        whole_blocks = 2 * rows_dev * route_count >= experts * rows_dev
        dense = whole_blocks and args[10].shape[0] == 1 and sp == 8 and tp == 4
        if not dense:
            return body(*args)
        return dense_body(*args)

    return jax.shard_map(
        chosen, mesh=mesh, in_specs=in_specs, out_specs=out_specs, check_vma=False
    )
```

```python
from functools import partial

import jax
import jax.numpy as jnp
from jax import lax
from jax.experimental import pallas as pl
from jax.experimental.pallas import tpu as pltpu
from jax.sharding import PartitionSpec as P

norm_eps = 1e-06
lowest_score = -1e30


def slot_targets(block_routes, experts, capacity):
    flat_routes = block_routes.reshape(-1)
    onehot = (flat_routes[:, None] == jnp.arange(experts, dtype=jnp.int32)[None, :]).astype(
        jnp.int32
    )
    earlier = jnp.cumsum(onehot, axis=0) - onehot
    return flat_routes * capacity + jnp.sum(earlier * onehot, axis=1)


def build_buffer(token_rows, block_routes, experts, capacity):
    targets = slot_targets(block_routes, experts, capacity)
    row_total = block_routes.shape[0]
    route_count = block_routes.shape[1]
    source_row = jnp.arange(row_total * route_count, dtype=jnp.int32) // route_count
    holder = jnp.full((experts * capacity,), row_total, jnp.int32).at[targets].set(source_row)
    padded = jnp.concatenate(
        [token_rows, jnp.zeros((1, token_rows.shape[1]), token_rows.dtype)], axis=0
    )
    return (padded[holder], targets)


def attention_block(carried, queries, key_block, value_block, score_scale):
    run_max, run_sum, accumulated = carried
    kv_local = run_max.shape[0]
    key_heads = key_block.reshape(key_block.shape[0], kv_local, 2, -1)
    value_heads = value_block.reshape(value_block.shape[0], kv_local, -1)
    scores = (
        jnp.einsum("qagcd,racd->agcqr", queries, key_heads, preferred_element_type=jnp.float32)
        * score_scale
    )
    new_max = jnp.maximum(run_max, jnp.max(scores, axis=-1))
    rescale = jnp.exp(run_max - new_max)
    weights = jnp.exp(scores - new_max[..., None])
    run_sum = run_sum * rescale + jnp.sum(weights, axis=-1)
    update = jnp.einsum(
        "agcqr,rae->agcqe",
        weights.astype(jnp.bfloat16),
        value_heads,
        preferred_element_type=jnp.float32,
    )
    return (new_max, run_sum, accumulated * rescale[..., None] + update)


def fold_keys(carried, pieces, first_row, queries, score_scale):
    key_piece, value_piece = pieces
    total_rows = key_piece.shape[0]
    block_rows = total_rows
    for candidate in (2048, 1024, 512):
        if total_rows % candidate == 0:
            block_rows = candidate
            break
    block_count = total_rows // block_rows

    def block_step(block_index, running):
        start_row = block_index * block_rows
        return attention_block(
            running,
            queries,
            lax.dynamic_slice_in_dim(key_piece, start_row, block_rows, 0),
            lax.dynamic_slice_in_dim(value_piece, start_row, block_rows, 0),
            score_scale,
        )

    return lax.fori_loop(0, block_count, block_step, carried)


def whole_experts(arrived, whole_gate, whole_up, whole_down, senders, capacity, groups):
    local_experts = whole_gate.shape[0]
    width = arrived.shape[-1]
    rows_in = arrived.reshape(senders, local_experts, capacity, width)
    gate_value = jnp.einsum(
        "sjtd,jdf->sjtf", rows_in, whole_gate, preferred_element_type=jnp.float32
    )
    up_value = jnp.einsum("sjtd,jdf->sjtf", rows_in, whole_up, preferred_element_type=jnp.float32)
    hidden = (jax.nn.silu(gate_value) * up_value).astype(jnp.bfloat16)
    hidden_units = hidden.shape[-1]
    hidden = hidden.reshape(senders, local_experts, capacity, groups, hidden_units // groups)
    down_groups = whole_down.reshape(local_experts, groups, hidden_units // groups, width)
    group_sums = jnp.einsum(
        "sjtgf,jgfd->sjtgd", hidden, down_groups, preferred_element_type=jnp.float32
    )
    group_sums = lax.optimization_barrier(group_sums.astype(jnp.bfloat16)).astype(jnp.float32)
    return (
        jnp.sum(group_sums, axis=3)
        .astype(jnp.bfloat16)
        .reshape(senders * local_experts * capacity, width)
    )


def body(
    query_maps,
    key_maps,
    value_rows,
    mix_lambda,
    head_gain,
    out_weight,
    residual,
    norm_gain,
    routes,
    route_weight,
    expert_gate,
    expert_up,
    expert_down,
    shared_gate,
    shared_up,
    shared_down,
):
    local_heads = mix_lambda.shape[0]
    head_width = head_gain.shape[0]
    kv_local = value_rows.shape[1] // head_width
    head_group = local_heads // kv_local
    head_dim = key_maps.shape[1] // (2 * kv_local)
    token_count = query_maps.shape[0]
    queries = query_maps.reshape(token_count, kv_local, head_group, 2, head_dim)
    start_max = jnp.full((kv_local, head_group, 2, token_count), lowest_score, jnp.float32)
    start_sum = jnp.zeros((kv_local, head_group, 2, token_count), jnp.float32)
    start_values = jnp.zeros((kv_local, head_group, 2, token_count, head_width), jnp.float32)
    folder = partial(fold_keys, queries=queries, score_scale=head_dim ** (-0.5))
    _, run_sum, accumulated = folder(
        (start_max, start_sum, start_values),
        (
            lax.all_gather(key_maps, "sp", axis=0, tiled=True),
            lax.all_gather(value_rows, "sp", axis=0, tiled=True),
        ),
        jnp.int32(0),
    )
    normalized = accumulated / run_sum[..., None]
    lambdas = mix_lambda.reshape(kv_local, head_group, 1, 1)
    difference = normalized[:, :, 0] - lambdas * normalized[:, :, 1]
    inverse_rms = lax.rsqrt(jnp.mean(difference * difference, axis=-1, keepdims=True) + norm_eps)
    head_scaled = (difference * inverse_rms * head_gain).astype(jnp.bfloat16)
    attended = jnp.transpose(head_scaled, (2, 0, 1, 3)).reshape(
        token_count, local_heads * head_width
    )
    columns = lax.axis_size("tp")
    column = lax.axis_index("tp")
    rows_dev = token_count // columns
    own_rows = lax.dynamic_slice_in_dim(
        out_weight, column * attended.shape[1], attended.shape[1], 0
    )
    projected = lax.psum_scatter(
        jnp.dot(attended, own_rows, preferred_element_type=jnp.float32).astype(jnp.bfloat16),
        "tp",
        scatter_dimension=0,
        tiled=True,
    ).astype(jnp.float32)
    stream = (residual.astype(jnp.float32) + projected).astype(jnp.bfloat16)
    stream_wide = stream.astype(jnp.float32)
    stream_rms = lax.rsqrt(jnp.mean(stream_wide * stream_wide, axis=1, keepdims=True) + norm_eps)
    normed = (stream_wide * stream_rms * norm_gain).astype(jnp.bfloat16)
    senders = lax.axis_size("sp")
    local_experts = expert_gate.shape[0]
    experts = senders * local_experts
    route_count = routes.shape[1]
    capacity = max(2, 2 * rows_dev * route_count // experts)
    local_routed = None
    whole_gate, whole_up, whole_down = (
        lax.all_gather(expert_gate, "tp", axis=2, tiled=True),
        lax.all_gather(expert_up, "tp", axis=2, tiled=True),
        lax.all_gather(expert_down, "tp", axis=1, tiled=True),
    )
    own_routes = lax.dynamic_slice_in_dim(routes, column * rows_dev, rows_dev, 0)
    buffer, targets = build_buffer(normed, own_routes, experts, capacity)
    arrived = lax.all_to_all(buffer, "sp", split_axis=0, concat_axis=0, tiled=True)
    local_routed = whole_experts(
        arrived, whole_gate, whole_up, whole_down, senders, capacity, columns
    )
    shared_rows = lax.all_gather(normed[None], "tp", axis=0, tiled=True)
    shared_in = shared_rows
    shared_in = shared_in.reshape(1 * lax.axis_size("tp") * rows_dev, shared_in.shape[-1])
    shared_hidden = (
        jax.nn.silu(jnp.dot(shared_in, shared_gate, preferred_element_type=jnp.float32))
        * jnp.dot(shared_in, shared_up, preferred_element_type=jnp.float32)
    ).astype(jnp.bfloat16)
    shared_out = jnp.dot(shared_hidden, shared_down, preferred_element_type=jnp.float32)
    pieces = shared_out.reshape(1 * lax.axis_size("tp"), rows_dev, shared_out.shape[-1])
    terms_out = pieces.astype(jnp.bfloat16)
    summed = (
        lax.psum_scatter(
            lax.optimization_barrier(terms_out).astype(jnp.float32).astype(jnp.bfloat16),
            "tp",
            scatter_dimension=0,
            tiled=True,
        )
        .astype(jnp.float32)[0]
        .astype(jnp.bfloat16)
    )
    returned = lax.all_to_all(local_routed, "sp", split_axis=0, concat_axis=0, tiled=True)
    picked = (
        returned[targets].reshape(rows_dev, route_count, returned.shape[-1]).astype(jnp.float32)
    )
    routed_sum = jnp.sum(route_weight[:, :, None] * picked, axis=1)
    return (stream_wide + summed.astype(jnp.float32) + routed_sum).astype(jnp.bfloat16)


MESH = pl.DeviceIdType.MESH


def peer_barrier(peers):
    barrier = pltpu.get_barrier_semaphore()
    for peer in peers:
        pl.semaphore_signal(barrier, inc=1, device_id=peer, device_id_type=MESH)
    pl.semaphore_wait(barrier, len(peers))


def remote(src, dst, send_sem, recv_sem, peer):
    return pltpu.make_async_remote_copy(
        src_ref=src,
        dst_ref=dst,
        send_sem=send_sem,
        recv_sem=recv_sem,
        device_id=peer,
        device_id_type=MESH,
    )


def grid_place(sp):
    s = lax.axis_index("sp")
    t = lax.axis_index("tp")
    return s, t, s // 2, s % 2, sp // 2


def whole_kernel(sp, tp, *refs):
    lam_ref, query_ref, key_ref, value_ref, table_ref = refs[:5]
    residual_ref, head_gain_ref, norm_gain_ref = refs[5:8]
    out_weight, own_gate, own_up, own_sgate, own_sup, own_sdown, own_down = refs[8:15]
    out_ref = refs[15]
    kbuf, vbuf, qbuf, run_max, run_sum, run_acc, att_out, att_in, proj = refs[16:25]
    normed_ref, stream_ref, tab_in = refs[25:28]
    gate, up, down, sgate, sup, sdown = refs[28:34]
    rows, hid_own, hid_out, hid_in, parts, xin, zout, zin, sout, sin, total = refs[34:45]
    zs, zr, xs, xr, ys, yr, hs, hr, os_, or_, rs, rr, ss, sr = refs[45:59]
    kzs, kzr, kxs, kxr, hes, her, ns, nr, fs, fr, gs, gr, ts, tr, wsem = refs[59:]
    s, t, z, x, depth = grid_place(sp)
    count, width = normed_ref.shape
    quarter = own_gate.shape[1]
    tokens, lanes = key_ref.shape
    head_group = lam_ref.shape[0]
    y, c = t // 2, t % 2
    across = (z * 2 + (1 - x), t)
    mirror = (s, (1 - y) * 2 + c)
    partner = (s, y * 2 + 1 - c)
    opposite = (s, (1 - y) * 2 + 1 - c)
    line = [(lax.rem(z + k, depth) * 2 + x, t) for k in range(1, depth)]
    far_line = [(lax.rem(z + k, depth) * 2 + 1 - x, t) for k in range(1, depth)]
    first, second = pl.ds(0, quarter), pl.ds(quarter, quarter)
    started = []

    def send(source, target, send_sem, recv_sem, peer):
        copy = remote(source, target, send_sem, recv_sem, peer)
        copy.start()
        started.append(copy)
        return copy

    loads = [
        pltpu.make_async_copy(source, place, wsem.at[n])
        for n, (source, place) in enumerate(
            (
                (own_gate, gate.at[:, first]),
                (own_up, up.at[:, first]),
                (own_sgate, sgate.at[:, first]),
                (own_sup, sup.at[:, first]),
                (own_sdown, sdown.at[first]),
                (own_down, down.at[first]),
                (out_weight, proj),
            )
        )
    ]
    peer_barrier(line + far_line + [across, mirror, partner, opposite])
    keys_z, keys_x = {}, {}

    def send_keys_x(j):
        sources = (key_ref, value_ref) if j == 0 else (kbuf.at[j, 0], vbuf.at[j, 0])
        keys_x[j] = [
            send(source, buf.at[j, 1], kxs.at[i, j], kxr.at[i, j], across)
            for i, (source, buf) in enumerate(zip(sources, (kbuf, vbuf)))
        ]

    slabs = [1, 3, 2] if depth == 4 else list(range(1, depth))
    send_keys_x(0)
    for j in slabs:
        k = depth - j
        keys_z[j] = [
            send(source, buf.at[j, 0], kzs.at[i, k - 1], kzr.at[i, k - 1], line[k - 1])
            for i, (source, buf) in enumerate(((key_ref, kbuf), (value_ref, vbuf)))
        ]
    for n in (6, 0, 1, 2, 3, 4, 5):
        loads[n].start()
    pieces = fs.shape[0]
    piece = quarter // pieces
    far_down = []

    def send_far(n):
        far_down.append(
            send(
                own_down.at[pl.ds(n * piece, piece)],
                down.at[pl.ds(2 * quarter + n * piece, piece)],
                fs.at[n],
                fr.at[n],
                mirror,
            )
        )

    for n in range(pieces - 1):
        send_far(n)
    near = [
        send(source, place, ns.at[n], nr.at[n], partner)
        for n, (source, place) in enumerate(
            (
                (own_gate, gate.at[:, second]),
                (own_up, up.at[:, second]),
                (own_sgate, sgate.at[:, second]),
                (own_sup, sup.at[:, second]),
                (own_sdown, sdown.at[second]),
                (own_down, down.at[second]),
            )
        )
    ]
    tab_in[s] = table_ref[...]
    tables = [
        send(table_ref, tab_in.at[s], ts.at[n], tr.at[n], peer)
        for n, peer in enumerate(line + far_line + [across])
    ]

    kbuf[0, 0] = key_ref[...]
    vbuf[0, 0] = value_ref[...]
    lane = lax.broadcasted_iota(jnp.int32, (tokens, lanes), 1)
    for a in range(head_group):
        head_query = query_ref[:, a * lanes : (a + 1) * lanes]
        for i in range(2):
            mine = (lane >= i * (lanes // 2)) & (lane < (i + 1) * (lanes // 2))
            qbuf[2 * a + i] = jnp.where(mine, head_query, jnp.zeros_like(head_query))
    scale = (lanes // 2) ** (-0.5)

    def attend(j):
        for copy in keys_x[j]:
            copy.wait_recv()
        keys = kbuf[j].reshape(2 * tokens, lanes)
        values = vbuf[j].reshape(2 * tokens, vbuf.shape[3])
        for m in range(2 * head_group):
            scores = scale * lax.dot_general(
                qbuf[m], keys, (((1,), (1,)), ((), ())), preferred_element_type=jnp.float32
            )
            top = jnp.max(scores, axis=1, keepdims=True)
            if j != 0:
                old = run_max[m]
                top = jnp.maximum(old, top)
                shrink = jnp.exp(old - top)
            weights = jnp.exp(scores - top)
            row_sum = jnp.sum(weights, axis=1, keepdims=True)
            update = jnp.dot(
                weights.astype(jnp.bfloat16), values, preferred_element_type=jnp.float32
            )
            if j != 0:
                row_sum = row_sum + run_sum[m] * shrink
                update = update + run_acc[m] * shrink
            run_max[m] = top
            run_sum[m] = row_sum
            run_acc[m] = update

    def relay_keys(j):
        for copy in keys_z[j]:
            copy.wait_recv()
        send_keys_x(j)

    relay_keys(slabs[0])
    attend(0)
    relay_keys(slabs[1])
    attend(slabs[0])
    relay_keys(slabs[2])
    attend(slabs[1])
    attend(slabs[2])
    for a in range(head_group):
        value = run_acc[2 * a] / run_sum[2 * a] - lam_ref[a] * (
            run_acc[2 * a + 1] / run_sum[2 * a + 1]
        )
        rms = lax.rsqrt(jnp.mean(value * value, axis=1, keepdims=True) + norm_eps)
        att_out[a] = (value * rms * head_gain_ref[...]).astype(jnp.bfloat16)
    heads = [
        send(
            att_out.at[:, pl.ds(pl.multiple_of(peer[1] * count, 16), count)],
            att_in.at[pl.ds(head_group * t, head_group)],
            hes.at[n],
            her.at[n],
            peer,
        )
        for n, peer in enumerate((mirror, opposite, partner))
    ]
    send_far(pieces - 1)
    att_in[pl.ds(head_group * t, head_group)] = att_out[
        :, pl.ds(pl.multiple_of(t * count, 16), count)
    ]
    loads[6].wait()
    for copy in heads:
        copy.wait_recv()
    attended = jnp.concatenate([att_in[h] for h in range(tp * head_group)], axis=1)
    stream = (
        residual_ref[...].astype(jnp.float32)
        + jnp.dot(attended, proj[...], preferred_element_type=jnp.float32)
    ).astype(jnp.bfloat16)
    stream_ref[...] = stream
    wide = stream.astype(jnp.float32)
    inverse = lax.rsqrt(jnp.mean(wide * wide, axis=1, keepdims=True) + norm_eps)
    normed_ref[...] = (wide * inverse * norm_gain_ref[...]).astype(jnp.bfloat16)

    z_rows = {}
    x_rows, y_rows, diagonal, hids, x_outs, z_outs = {}, {}, {}, {}, {}, {}

    def own_rows(j):
        return normed_ref if j == 0 else rows.at[0, j, 0]

    def hidden_of(block, gate_buf, up_buf):
        gate_value = jnp.dot(block, gate_buf[...], preferred_element_type=jnp.float32)
        up_value = jnp.dot(block, up_buf[...], preferred_element_type=jnp.float32)
        return (jax.nn.silu(gate_value) * up_value).astype(jnp.bfloat16)

    waited = set()

    def arrived(copies, j):
        if (id(copies), j) not in waited:
            waited.add((id(copies), j))
            copies[j].wait_recv()

    def loaded(first_load, last_load):
        for n in range(first_load, last_load):
            if ("load", n) not in waited:
                waited.add(("load", n))
                loads[n].wait()
                near[n].wait_recv()

    def RX(j):
        if j != 0:
            arrived(z_rows, j)
        x_rows[j] = send(own_rows(j), rows.at[0, j, 1], xs.at[j], xr.at[j], across)

    def RY(j):
        if j != 0:
            arrived(z_rows, j)
        y_rows[j] = send(own_rows(j), rows.at[1, j, 0], ys.at[j], yr.at[j], mirror)

    def RD(j):
        sems = ys.at[depth + j], yr.at[depth + j]
        if j in by_x:
            arrived(y_rows, j)
            diagonal[j] = send(rows.at[1, j, 0], rows.at[1, j, 1], *sems, across)
        else:
            arrived(x_rows, j)
            diagonal[j] = send(rows.at[0, j, 1], rows.at[1, j, 1], *sems, mirror)

    def HO(j):
        arrived(x_rows, j)
        loaded(0, 2)
        hid_own[j] = hidden_of(rows[0, j].reshape(2 * count, width), gate, up)

    def HP(j):
        arrived(y_rows, j)
        arrived(diagonal, j)
        loaded(0, 2)
        hid_out[j] = hidden_of(rows[1, j].reshape(2 * count, width), gate, up)
        hids[j] = send(hid_out.at[j], hid_in.at[j], hs.at[j], hr.at[j], mirror)

    far_near = []

    def DR(j):
        for n, copy in enumerate(far_down):
            copy.wait_recv()
            far_near.append(
                send(
                    down.at[pl.ds(2 * quarter + n * piece, piece)],
                    down.at[pl.ds(3 * quarter + n * piece, piece)],
                    gs.at[n],
                    gr.at[n],
                    partner,
                )
            )

    def route_column(source):
        row = tab_in[source, pl.ds(s, 1)]
        shape = (count, row.shape[1])
        diagonal_mask = lax.broadcasted_iota(jnp.int32, shape, 0) == lax.broadcasted_iota(
            jnp.int32, shape, 1
        )
        spread = jnp.broadcast_to(row, shape)
        return jnp.sum(jnp.where(diagonal_mask, spread, 0.0), axis=1, keepdims=True)

    def FD(j):
        loaded(5, 6)
        for copies in (far_near, tables):
            if ("all", id(copies)) not in waited:
                waited.add(("all", id(copies)))
                for copy in copies:
                    copy.wait_recv()
        arrived(hids, j)
        half = hid_own.shape[2]
        value = jnp.dot(
            hid_own[j], down[pl.ds(0, half)], preferred_element_type=jnp.float32
        ) + jnp.dot(hid_in[j], down[pl.ds(half, half)], preferred_element_type=jnp.float32)
        base = lax.rem(z + j, depth) * 2
        parts[j, 1] = (value[count:] * route_column(base + 1 - x)).astype(jnp.bfloat16)
        x_outs[j] = send(parts.at[j, 1], xin.at[j], os_.at[j], or_.at[j], across)
        parts[j, 0] = (value[:count] * route_column(base + x)).astype(jnp.bfloat16)

    def FO(j):
        arrived(x_outs, j)
        zout[j - 1] = (parts[j, 0].astype(jnp.float32) + xin[j].astype(jnp.float32)).astype(
            jnp.bfloat16
        )
        z_outs[j] = send(
            zout.at[j - 1], zin.at[j - 1], rs.at[j - 1], rr.at[j - 1], line[j - 1]
        )

    shared_copy = []

    def SH(j):
        arrived(y_rows, 0)
        loaded(2, 5)
        pair = jnp.concatenate([normed_ref[...], rows[1, 0, 0]], axis=0)
        shared = jnp.dot(
            hidden_of(pair, sgate, sup), sdown[...], preferred_element_type=jnp.float32
        )
        sout[...] = shared[count:].astype(jnp.bfloat16)
        total[...] = stream_ref[...].astype(jnp.float32) + shared[:count]

    def SS(j):
        shared_copy.append(send(sout, sin, ss, sr, mirror))

    actions = {f.__name__: f for f in (RX, RY, RD, HO, HP, FD, FO, SH, SS, DR)}
    by_x, steps = moe_plan()
    rows[0, 0, 0] = normed_ref[...]
    for j in slabs:
        k = depth - j
        z_rows[j] = send(
            normed_ref, rows.at[0, j, 0], zs.at[k - 1], zr.at[k - 1], line[k - 1]
        )
    for step in steps:
        actions[step[:2]](int(step[2:] or 0))
    shared_copy[0].wait_recv()
    arrived(x_outs, 0)
    value = total[...] + sin[...].astype(jnp.float32)
    value = value + parts[0, 0].astype(jnp.float32) + xin[0].astype(jnp.float32)
    for j in range(1, depth):
        arrived(z_outs, j)
        value = value + zin[j - 1].astype(jnp.float32)
    out_ref[...] = value.astype(out_ref.dtype)
    for copy in started:
        copy.wait_send()


def moe_plan():
    return (0, 3), [
        step
        for group in (
            "RY0 RX0 RY1 RX1",
            "RY3 RX3 HO1 RD1",
            "RX2 RY2 RD3 HP1",
            "RD0 RD2 HO3 DR",
            "HP3",
            "FD1 HP2 FD3 FO1",
            "HP0 HO2 FD2 FO3",
            "HO0 FD0 FO2 SH",
            "SS",
        )
        for step in group.split()
    ]


def run_whole(scalars, small, large, tp, sp, collective_id):
    _, key, value, table, residual = small[:5]
    count, width = residual.shape
    tokens, lanes = key.shape
    head_group = scalars.shape[0]
    depth = sp // 2
    quarter = large[1].shape[1]
    half = 2 * quarter
    bf16, f32 = jnp.bfloat16, jnp.float32
    vmem = pl.BlockSpec(memory_space=pltpu.VMEM)
    pieces = 4

    def dma(*shape):
        return [pltpu.SemaphoreType.DMA(shape)] * 2

    maps = 2 * head_group
    scratch = [
        ((depth, 2, tokens, lanes), bf16),
        ((depth, 2, tokens, value.shape[1]), bf16),
        ((maps, tokens, lanes), bf16),
        ((maps, tokens, 1), f32),
        ((maps, tokens, 1), f32),
        ((maps, tokens, value.shape[1]), f32),
        ((head_group, tokens, value.shape[1]), bf16),
        ((tp * head_group, count, value.shape[1]), bf16),
        (large[0].shape, bf16),
        ((count, width), bf16),
        ((count, width), bf16),
        ((sp,) + table.shape, f32),
        ((width, half), bf16),
        ((width, half), bf16),
        ((2 * half, width), bf16),
        ((width, half), bf16),
        ((width, half), bf16),
        ((half, width), bf16),
        ((2, depth, 2, count, width), bf16),
        ((depth, 2 * count, half), bf16),
        ((depth, 2 * count, half), bf16),
        ((depth, 2 * count, half), bf16),
        ((depth, 2, count, width), bf16),
        ((depth, count, width), bf16),
        ((depth - 1, count, width), bf16),
        ((depth - 1, count, width), bf16),
        ((count, width), bf16),
        ((count, width), bf16),
        ((count, width), f32),
    ]
    return pl.pallas_call(
        partial(whole_kernel, sp, tp),
        out_shape=jax.ShapeDtypeStruct((count, width), bf16),
        in_specs=[pl.BlockSpec(memory_space=pltpu.SMEM)]
        + [vmem] * len(small)
        + [pl.BlockSpec(memory_space=pl.ANY)] * len(large),
        out_specs=vmem,
        scratch_shapes=[pltpu.VMEM(shape, dtype) for shape, dtype in scratch]
        + dma(depth - 1)
        + dma(depth)
        + dma(2 * depth)
        + dma(depth)
        + dma(depth)
        + dma(depth - 1)
        + [pltpu.SemaphoreType.DMA] * 2
        + dma(2, depth - 1)
        + dma(2, depth)
        + dma(tp - 1)
        + dma(6)
        + dma(pieces)
        + dma(pieces)
        + dma(sp - 1)
        + [pltpu.SemaphoreType.DMA((len(large),))],
        compiler_params=pltpu.CompilerParams(
            collective_id=collective_id,
            has_side_effects=True,
            vmem_limit_bytes=58 * 1024 * 1024,
        ),
        cost_estimate=pl.CostEstimate(
            flops=12 * depth * count * width * half * 3,
            bytes_accessed=30_000_000,
            transcendentals=0,
        ),
    )(scalars, *small, *large)


def dense_body(
    query_maps,
    key_maps,
    value_rows,
    mix_lambda,
    head_gain,
    out_weight,
    residual,
    norm_gain,
    routes,
    route_weight,
    expert_gate,
    expert_up,
    expert_down,
    shared_gate,
    shared_up,
    shared_down,
):
    sp = lax.axis_size("sp")
    tp = lax.axis_size("tp")
    t = lax.axis_index("tp")
    head_width = head_gain.shape[0]
    rows_dev = residual.shape[0]
    width = residual.shape[1]
    own_routes = lax.dynamic_slice_in_dim(routes, t * rows_dev, rows_dev, 0)
    named = own_routes[None, :, :] == jnp.arange(sp, dtype=jnp.int32)[:, None, None]
    table = jnp.sum(jnp.where(named, route_weight[None], 0.0), axis=2)
    lanes = -(-rows_dev // 128) * 128
    table = jnp.pad(table, ((0, 0), (0, lanes - rows_dev)))
    return run_whole(
        mix_lambda,
        (
            query_maps,
            key_maps,
            value_rows,
            table,
            residual,
            head_gain.reshape(1, head_width),
            norm_gain.reshape(1, width),
        ),
        (
            out_weight,
            expert_gate[0],
            expert_up[0],
            shared_gate,
            shared_up,
            shared_down,
            expert_down[0],
        ),
        tp,
        sp,
        1,
    )


def solution(mesh):
    in_specs = (
        P("sp", "tp"),
        P("sp", "tp"),
        P("sp", "tp"),
        P("tp"),
        P(),
        P(),
        P(("sp", "tp"), None),
        P(),
        P("sp", None),
        P(("sp", "tp"), None),
        P("sp", None, "tp"),
        P("sp", None, "tp"),
        P("sp", "tp", None),
        P(None, "tp"),
        P(None, "tp"),
        P("tp", None),
    )
    out_specs = P(("sp", "tp"), None)
    sp, tp = mesh.shape["sp"], mesh.shape["tp"]

    def chosen(*args):
        route_count = args[8].shape[1]
        experts = sp * args[10].shape[0]
        rows_dev = args[6].shape[0]
        whole_blocks = 2 * rows_dev * route_count >= experts * rows_dev
        kv_local = args[2].shape[1] // args[4].shape[0]
        dense = whole_blocks and args[10].shape[0] == 1 and sp == 8 and tp == 4 and kv_local == 1
        if not dense:
            return body(*args)
        return dense_body(*args)

    return jax.shard_map(
        chosen, mesh=mesh, in_specs=in_specs, out_specs=out_specs, check_vma=False
    )
```

```python
from functools import partial

import jax
import jax.numpy as jnp
from jax import lax
from jax.experimental import pallas as pl
from jax.experimental.pallas import tpu as pltpu
from jax.sharding import PartitionSpec as P

norm_eps = 1e-06
lowest_score = -1e30


def slot_targets(block_routes, experts, capacity):
    flat_routes = block_routes.reshape(-1)
    onehot = (flat_routes[:, None] == jnp.arange(experts, dtype=jnp.int32)[None, :]).astype(
        jnp.int32
    )
    earlier = jnp.cumsum(onehot, axis=0) - onehot
    return flat_routes * capacity + jnp.sum(earlier * onehot, axis=1)


def build_buffer(token_rows, block_routes, experts, capacity):
    targets = slot_targets(block_routes, experts, capacity)
    row_total = block_routes.shape[0]
    route_count = block_routes.shape[1]
    source_row = jnp.arange(row_total * route_count, dtype=jnp.int32) // route_count
    holder = jnp.full((experts * capacity,), row_total, jnp.int32).at[targets].set(source_row)
    padded = jnp.concatenate(
        [token_rows, jnp.zeros((1, token_rows.shape[1]), token_rows.dtype)], axis=0
    )
    return (padded[holder], targets)


def attention_block(carried, queries, key_block, value_block, score_scale):
    run_max, run_sum, accumulated = carried
    kv_local = run_max.shape[0]
    key_heads = key_block.reshape(key_block.shape[0], kv_local, 2, -1)
    value_heads = value_block.reshape(value_block.shape[0], kv_local, -1)
    scores = (
        jnp.einsum("qagcd,racd->agcqr", queries, key_heads, preferred_element_type=jnp.float32)
        * score_scale
    )
    new_max = jnp.maximum(run_max, jnp.max(scores, axis=-1))
    rescale = jnp.exp(run_max - new_max)
    weights = jnp.exp(scores - new_max[..., None])
    run_sum = run_sum * rescale + jnp.sum(weights, axis=-1)
    update = jnp.einsum(
        "agcqr,rae->agcqe",
        weights.astype(jnp.bfloat16),
        value_heads,
        preferred_element_type=jnp.float32,
    )
    return (new_max, run_sum, accumulated * rescale[..., None] + update)


def fold_keys(carried, pieces, first_row, queries, score_scale):
    key_piece, value_piece = pieces
    total_rows = key_piece.shape[0]
    block_rows = total_rows
    for candidate in (2048, 1024, 512):
        if total_rows % candidate == 0:
            block_rows = candidate
            break
    block_count = total_rows // block_rows

    def block_step(block_index, running):
        start_row = block_index * block_rows
        return attention_block(
            running,
            queries,
            lax.dynamic_slice_in_dim(key_piece, start_row, block_rows, 0),
            lax.dynamic_slice_in_dim(value_piece, start_row, block_rows, 0),
            score_scale,
        )

    return lax.fori_loop(0, block_count, block_step, carried)


def whole_experts(arrived, whole_gate, whole_up, whole_down, senders, capacity, groups):
    local_experts = whole_gate.shape[0]
    width = arrived.shape[-1]
    rows_in = arrived.reshape(senders, local_experts, capacity, width)
    gate_value = jnp.einsum(
        "sjtd,jdf->sjtf", rows_in, whole_gate, preferred_element_type=jnp.float32
    )
    up_value = jnp.einsum("sjtd,jdf->sjtf", rows_in, whole_up, preferred_element_type=jnp.float32)
    hidden = (jax.nn.silu(gate_value) * up_value).astype(jnp.bfloat16)
    hidden_units = hidden.shape[-1]
    hidden = hidden.reshape(senders, local_experts, capacity, groups, hidden_units // groups)
    down_groups = whole_down.reshape(local_experts, groups, hidden_units // groups, width)
    group_sums = jnp.einsum(
        "sjtgf,jgfd->sjtgd", hidden, down_groups, preferred_element_type=jnp.float32
    )
    group_sums = lax.optimization_barrier(group_sums.astype(jnp.bfloat16)).astype(jnp.float32)
    return (
        jnp.sum(group_sums, axis=3)
        .astype(jnp.bfloat16)
        .reshape(senders * local_experts * capacity, width)
    )


def body(
    query_maps,
    key_maps,
    value_rows,
    mix_lambda,
    head_gain,
    out_weight,
    residual,
    norm_gain,
    routes,
    route_weight,
    expert_gate,
    expert_up,
    expert_down,
    shared_gate,
    shared_up,
    shared_down,
):
    local_heads = mix_lambda.shape[0]
    head_width = head_gain.shape[0]
    kv_local = value_rows.shape[1] // head_width
    head_group = local_heads // kv_local
    head_dim = key_maps.shape[1] // (2 * kv_local)
    token_count = query_maps.shape[0]
    queries = query_maps.reshape(token_count, kv_local, head_group, 2, head_dim)
    start_max = jnp.full((kv_local, head_group, 2, token_count), lowest_score, jnp.float32)
    start_sum = jnp.zeros((kv_local, head_group, 2, token_count), jnp.float32)
    start_values = jnp.zeros((kv_local, head_group, 2, token_count, head_width), jnp.float32)
    folder = partial(fold_keys, queries=queries, score_scale=head_dim ** (-0.5))
    _, run_sum, accumulated = folder(
        (start_max, start_sum, start_values),
        (
            lax.all_gather(key_maps, "sp", axis=0, tiled=True),
            lax.all_gather(value_rows, "sp", axis=0, tiled=True),
        ),
        jnp.int32(0),
    )
    normalized = accumulated / run_sum[..., None]
    lambdas = mix_lambda.reshape(kv_local, head_group, 1, 1)
    difference = normalized[:, :, 0] - lambdas * normalized[:, :, 1]
    inverse_rms = lax.rsqrt(jnp.mean(difference * difference, axis=-1, keepdims=True) + norm_eps)
    head_scaled = (difference * inverse_rms * head_gain).astype(jnp.bfloat16)
    attended = jnp.transpose(head_scaled, (2, 0, 1, 3)).reshape(
        token_count, local_heads * head_width
    )
    columns = lax.axis_size("tp")
    column = lax.axis_index("tp")
    rows_dev = token_count // columns
    own_rows = lax.dynamic_slice_in_dim(
        out_weight, column * attended.shape[1], attended.shape[1], 0
    )
    projected = lax.psum_scatter(
        jnp.dot(attended, own_rows, preferred_element_type=jnp.float32).astype(jnp.bfloat16),
        "tp",
        scatter_dimension=0,
        tiled=True,
    ).astype(jnp.float32)
    stream = (residual.astype(jnp.float32) + projected).astype(jnp.bfloat16)
    stream_wide = stream.astype(jnp.float32)
    stream_rms = lax.rsqrt(jnp.mean(stream_wide * stream_wide, axis=1, keepdims=True) + norm_eps)
    normed = (stream_wide * stream_rms * norm_gain).astype(jnp.bfloat16)
    senders = lax.axis_size("sp")
    local_experts = expert_gate.shape[0]
    experts = senders * local_experts
    route_count = routes.shape[1]
    capacity = max(2, 2 * rows_dev * route_count // experts)
    local_routed = None
    whole_gate, whole_up, whole_down = (
        lax.all_gather(expert_gate, "tp", axis=2, tiled=True),
        lax.all_gather(expert_up, "tp", axis=2, tiled=True),
        lax.all_gather(expert_down, "tp", axis=1, tiled=True),
    )
    own_routes = lax.dynamic_slice_in_dim(routes, column * rows_dev, rows_dev, 0)
    buffer, targets = build_buffer(normed, own_routes, experts, capacity)
    arrived = lax.all_to_all(buffer, "sp", split_axis=0, concat_axis=0, tiled=True)
    local_routed = whole_experts(
        arrived, whole_gate, whole_up, whole_down, senders, capacity, columns
    )
    shared_rows = lax.all_gather(normed[None], "tp", axis=0, tiled=True)
    shared_in = shared_rows
    shared_in = shared_in.reshape(1 * lax.axis_size("tp") * rows_dev, shared_in.shape[-1])
    shared_hidden = (
        jax.nn.silu(jnp.dot(shared_in, shared_gate, preferred_element_type=jnp.float32))
        * jnp.dot(shared_in, shared_up, preferred_element_type=jnp.float32)
    ).astype(jnp.bfloat16)
    shared_out = jnp.dot(shared_hidden, shared_down, preferred_element_type=jnp.float32)
    pieces = shared_out.reshape(1 * lax.axis_size("tp"), rows_dev, shared_out.shape[-1])
    terms_out = pieces.astype(jnp.bfloat16)
    summed = (
        lax.psum_scatter(
            lax.optimization_barrier(terms_out).astype(jnp.float32).astype(jnp.bfloat16),
            "tp",
            scatter_dimension=0,
            tiled=True,
        )
        .astype(jnp.float32)[0]
        .astype(jnp.bfloat16)
    )
    returned = lax.all_to_all(local_routed, "sp", split_axis=0, concat_axis=0, tiled=True)
    picked = (
        returned[targets].reshape(rows_dev, route_count, returned.shape[-1]).astype(jnp.float32)
    )
    routed_sum = jnp.sum(route_weight[:, :, None] * picked, axis=1)
    return (stream_wide + summed.astype(jnp.float32) + routed_sum).astype(jnp.bfloat16)


MESH = pl.DeviceIdType.MESH


def remote(src, dst, send_sem, recv_sem, peer):
    return pltpu.make_async_remote_copy(
        src_ref=src,
        dst_ref=dst,
        send_sem=send_sem,
        recv_sem=recv_sem,
        device_id=peer,
        device_id_type=MESH,
    )


def grid_place(sp):
    s = lax.axis_index("sp")
    t = lax.axis_index("tp")
    return s, t, s // 2, s % 2, sp // 2


def whole_kernel(sp, tp, *refs):
    inputs, small = refs[:9], refs[17:25]
    out_weight, own_gate, own_up, own_sgate, own_sup, own_sdown, own_down = refs[9:16]
    out_ref = refs[16]
    query_ref, lam_ref, routes_ref, route_weight_ref = small[:4]
    residual_ref, head_gain_ref, norm_gain_ref, table_ref = small[4:]
    kbuf, vbuf, qbuf, run_max, run_sum, run_acc, att_out, att_in, proj = refs[25:34]
    normed_ref, stream_ref, tab_in = refs[34:37]
    gate, up, down, sgate, sup, sdown = refs[37:43]
    rows, hid_own, hid_out, hid_in, parts, xin, zout, zin, sout, sin, total = refs[43:54]
    zs, zr, xs, xr, ys, yr, hs, hr, os_, or_, rs, rr, ss, sr = refs[54:68]
    kzs, kzr, kxs, kxr, hes, her, ns, nr, fs, fr, gs, gr, ts, tr, wsem, isem = refs[68:]
    s, t, z, x, depth = grid_place(sp)
    count, width = normed_ref.shape
    quarter = own_gate.shape[1]
    tokens, lanes = kbuf.shape[2:]
    head_group = lam_ref.shape[0]
    y, c = t // 2, t % 2
    across = (z * 2 + (1 - x), t)
    mirror = (s, (1 - y) * 2 + c)
    partner = (s, y * 2 + 1 - c)
    opposite = (s, (1 - y) * 2 + 1 - c)
    line = [(lax.rem(z + k, depth) * 2 + x, t) for k in range(1, depth)]
    far_line = [(lax.rem(z + k, depth) * 2 + 1 - x, t) for k in range(1, depth)]
    first, second = pl.ds(0, quarter), pl.ds(quarter, quarter)
    started = []

    def send(source, target, send_sem, recv_sem, peer):
        copy = remote(source, target, send_sem, recv_sem, peer)
        copy.start()
        started.append(copy)
        return copy

    loads = [
        pltpu.make_async_copy(source, place, wsem.at[n])
        for n, (source, place) in enumerate(
            (
                (own_gate, gate.at[:, first]),
                (own_up, up.at[:, first]),
                (own_sgate, sgate.at[:, first]),
                (own_sup, sup.at[:, first]),
                (own_sdown, sdown.at[first]),
                (own_down, down.at[first]),
                (out_weight, proj),
            )
        )
    ]
    peers = line + far_line + [across, mirror, partner, opposite]
    barrier = pltpu.get_barrier_semaphore()
    for peer in peers:
        pl.semaphore_signal(barrier, inc=1, device_id=peer, device_id_type=MESH)
    fetches = [
        pltpu.make_async_copy(source, place, isem.at[n])
        for n, (source, place) in enumerate(
            zip(
                inputs,
                (
                    kbuf.at[0, 0],
                    vbuf.at[0, 0],
                    query_ref,
                    lam_ref,
                    routes_ref,
                    route_weight_ref,
                    residual_ref,
                    head_gain_ref,
                    norm_gain_ref,
                ),
            )
        )
    ]
    for fetch in fetches:
        fetch.start()
    fetches[0].wait()
    fetches[1].wait()
    pl.semaphore_wait(barrier, len(peers))
    keys_z, keys_x = {}, {}

    def send_keys_x(j):
        keys_x[j] = [
            send(buf.at[j, 0], buf.at[j, 1], kxs.at[i, j], kxr.at[i, j], across)
            for i, buf in enumerate((kbuf, vbuf))
        ]

    slabs = [1, 3, 2] if depth == 4 else list(range(1, depth))
    send_keys_x(0)
    for j in slabs:
        k = depth - j
        keys_z[j] = [
            send(buf.at[0, 0], buf.at[j, 0], kzs.at[i, k - 1], kzr.at[i, k - 1], line[k - 1])
            for i, buf in enumerate((kbuf, vbuf))
        ]
    for n in (6, 0, 1, 2, 3, 4, 5):
        loads[n].start()
    pieces = fs.shape[0]
    early = pieces - 2
    piece = quarter // pieces
    far_down = []

    def send_far(n):
        far_down.append(
            send(
                own_down.at[pl.ds(n * piece, piece)],
                down.at[pl.ds(2 * quarter + n * piece, piece)],
                fs.at[n],
                fr.at[n],
                mirror,
            )
        )

    send_far(0)
    send_far(1)
    near = [
        send(source, place, ns.at[n], nr.at[n], partner)
        for n, (source, place) in enumerate(
            (
                (own_gate, gate.at[:, second]),
                (own_up, up.at[:, second]),
                (own_sgate, sgate.at[:, second]),
                (own_sup, sup.at[:, second]),
                (own_sdown, sdown.at[second]),
                (own_down, down.at[second]),
            )
        )
    ]
    for fetch in fetches[2:]:
        fetch.wait()
    lane = lax.broadcasted_iota(jnp.int32, (tokens, lanes), 1)
    for a in range(head_group):
        head_query = query_ref[:, a * lanes : (a + 1) * lanes]
        for i in range(2):
            mine = (lane >= i * (lanes // 2)) & (lane < (i + 1) * (lanes // 2))
            qbuf[2 * a + i] = jnp.where(mine, head_query, jnp.zeros_like(head_query))
    scale = (lanes // 2) ** (-0.5)

    def attend(j, low=0, high=2):
        if high == 2:
            for copy in keys_x[j]:
                copy.wait_recv()
        keys = kbuf[j, low:high].reshape((high - low) * tokens, lanes)
        values = vbuf[j, low:high].reshape((high - low) * tokens, vbuf.shape[3])
        for m in range(2 * head_group):
            scores = scale * lax.dot_general(
                qbuf[m], keys, (((1,), (1,)), ((), ())), preferred_element_type=jnp.float32
            )
            top = jnp.max(scores, axis=1, keepdims=True)
            if j != 0:
                old = run_max[m]
                top = jnp.maximum(old, top)
                shrink = jnp.exp(old - top)
            weights = jnp.exp(scores - top)
            row_sum = jnp.sum(weights, axis=1, keepdims=True)
            update = jnp.dot(
                weights.astype(jnp.bfloat16), values, preferred_element_type=jnp.float32
            )
            if j != 0:
                row_sum = row_sum + run_sum[m] * shrink
                update = update + run_acc[m] * shrink
            run_max[m] = top
            run_sum[m] = row_sum
            run_acc[m] = update

    def relay_keys(j):
        for copy in keys_z[j]:
            copy.wait_recv()
        send_keys_x(j)

    def build_table():
        chosen = routes_ref[:, :count]
        for n in range(1, tp):
            chosen = jnp.where(t == n, routes_ref[:, n * count : (n + 1) * count], chosen)
        names = [
            jnp.sum(
                jnp.where(chosen == expert, route_weight_ref[...], 0.0), axis=0, keepdims=True
            )
            for expert in range(sp)
        ]
        table = jnp.concatenate(names, axis=0)
        spare = jnp.zeros((sp, table_ref.shape[1] - count), jnp.float32)
        table_ref[...] = jnp.concatenate([table, spare], axis=1)
        tab_in[s] = table_ref[...]
        return [
            send(table_ref, tab_in.at[s], ts.at[n], tr.at[n], peer)
            for n, peer in enumerate(line + far_line + [across])
        ]

    relay_keys(slabs[0])
    send_far(2)
    attend(0)
    relay_keys(slabs[1])
    attend(slabs[0])
    send_far(3)
    relay_keys(slabs[2])
    attend(slabs[2], 0, 1)
    tables = build_table()
    attend(slabs[1])
    send_far(4)
    attend(slabs[2], 1, 2)
    for a in range(head_group):
        value = run_acc[2 * a] / run_sum[2 * a] - lam_ref[a] * (
            run_acc[2 * a + 1] / run_sum[2 * a + 1]
        )
        rms = lax.rsqrt(jnp.mean(value * value, axis=1, keepdims=True) + norm_eps)
        att_out[a] = (value * rms * head_gain_ref[...]).astype(jnp.bfloat16)
    heads = [
        send(
            att_out.at[:, pl.ds(pl.multiple_of(peer[1] * count, 16), count)],
            att_in.at[pl.ds(head_group * t, head_group)],
            hes.at[n],
            her.at[n],
            peer,
        )
        for n, peer in enumerate((mirror, opposite, partner))
    ]
    for n in range(5, early):
        send_far(n)
    att_in[pl.ds(head_group * t, head_group)] = att_out[
        :, pl.ds(pl.multiple_of(t * count, 16), count)
    ]
    loads[6].wait()
    for copy in heads:
        copy.wait_recv()
    attended = jnp.concatenate([att_in[h] for h in range(tp * head_group)], axis=1)
    stream = (
        residual_ref[...].astype(jnp.float32)
        + jnp.dot(attended, proj[...], preferred_element_type=jnp.float32)
    ).astype(jnp.bfloat16)
    stream_ref[...] = stream
    wide = stream.astype(jnp.float32)
    inverse = lax.rsqrt(jnp.mean(wide * wide, axis=1, keepdims=True) + norm_eps)
    normed_ref[...] = (wide * inverse * norm_gain_ref[...]).astype(jnp.bfloat16)

    z_rows = {}
    x_rows, y_rows, diagonal, hids, x_outs, z_outs = {}, {}, {}, {}, {}, {}
    half_width = width // 2
    waited = set()

    def part(ref, h):
        return ref.at[:, pl.ds(h * half_width, half_width)]

    def own_rows(j, h):
        return part(normed_ref if j == 0 else rows.at[0, j, 0], h)

    def hidden_of(block, gate_buf, up_buf):
        gate_value = jnp.dot(block, gate_buf[...], preferred_element_type=jnp.float32)
        up_value = jnp.dot(block, up_buf[...], preferred_element_type=jnp.float32)
        return (jax.nn.silu(gate_value) * up_value).astype(jnp.bfloat16)

    def arrived(copies, *keys):
        for key in keys:
            if (id(copies), key) not in waited:
                waited.add((id(copies), key))
                copies[key].wait_recv()

    def loaded(first_load, last_load):
        for n in range(first_load, last_load):
            if ("load", n) not in waited:
                waited.add(("load", n))
                loads[n].wait()
                near[n].wait_recv()

    def RX(j, h):
        if j != 0:
            arrived(z_rows, (j, h))
        x_rows[j, h] = send(
            own_rows(j, h), part(rows.at[0, j, 1], h), xs.at[j, h], xr.at[j, h], across
        )

    def RY(j, h):
        sems = ys.at[j, h], yr.at[j, h]
        if j in by_z:
            arrived(y_rows, (0, h))
            y_rows[j, h] = send(
                part(rows.at[1, 0, 0], h), part(rows.at[1, j, 0], h), *sems, line[depth - j - 1]
            )
            return
        if j != 0:
            arrived(z_rows, (j, h))
        y_rows[j, h] = send(own_rows(j, h), part(rows.at[1, j, 0], h), *sems, mirror)

    def RD(j, h):
        sems = ys.at[depth + j, h], yr.at[depth + j, h]
        target = part(rows.at[1, j, 1], h)
        if j in by_x:
            arrived(y_rows, (j, h))
            diagonal[j, h] = send(part(rows.at[1, j, 0], h), target, *sems, across)
        else:
            arrived(x_rows, (j, h))
            diagonal[j, h] = send(part(rows.at[0, j, 1], h), target, *sems, mirror)

    def HO(j, h):
        if j != 0:
            arrived(z_rows, (j, 0), (j, 1))
        arrived(x_rows, (j, 0), (j, 1))
        loaded(0, 2)
        hid_own[j] = hidden_of(rows[0, j].reshape(2 * count, width), gate, up)

    def HP(j, h):
        arrived(y_rows, (j, 0), (j, 1))
        arrived(diagonal, (j, 0), (j, 1))
        loaded(0, 2)
        hid_out[j] = hidden_of(rows[1, j].reshape(2 * count, width), gate, up)
        hids[j] = send(hid_out.at[j], hid_in.at[j], hs.at[j], hr.at[j], mirror)

    far_near = []

    def FR(j, h):
        for n in range(j, pieces):
            if n == j or h:
                send_far(n)

    def DR(j, h):
        for n, copy in enumerate(far_down):
            copy.wait_recv()
            far_near.append(
                send(
                    down.at[pl.ds(2 * quarter + n * piece, piece)],
                    down.at[pl.ds(3 * quarter + n * piece, piece)],
                    gs.at[n],
                    gr.at[n],
                    partner,
                )
            )

    def route_column(source):
        row = tab_in[source, pl.ds(s, 1)]
        shape = (count, row.shape[1])
        diagonal_mask = lax.broadcasted_iota(jnp.int32, shape, 0) == lax.broadcasted_iota(
            jnp.int32, shape, 1
        )
        spread = jnp.broadcast_to(row, shape)
        return jnp.sum(jnp.where(diagonal_mask, spread, 0.0), axis=1, keepdims=True)

    def FD(j, h):
        loaded(5, 6)
        for copies in (far_near, tables):
            if ("all", id(copies)) not in waited:
                waited.add(("all", id(copies)))
                for copy in copies:
                    copy.wait_recv()
        arrived(hids, j)
        half = hid_own.shape[2]
        columns = pl.ds(h * half_width, half_width)
        value = jnp.dot(
            hid_own[j], down[pl.ds(0, half), columns], preferred_element_type=jnp.float32
        ) + jnp.dot(
            hid_in[j], down[pl.ds(half, half), columns], preferred_element_type=jnp.float32
        )
        base = lax.rem(z + j, depth) * 2
        parts[j, 1, :, columns] = (value[count:] * route_column(base + 1 - x)).astype(
            jnp.bfloat16
        )
        x_outs[j, h] = send(
            part(parts.at[j, 1], h), part(xin.at[j], h), os_.at[j, h], or_.at[j, h], across
        )
        parts[j, 0, :, columns] = (value[:count] * route_column(base + x)).astype(jnp.bfloat16)

    def FO(j, h):
        arrived(x_outs, (j, h))
        columns = pl.ds(h * half_width, half_width)
        zout[j - 1, :, columns] = (
            parts[j, 0, :, columns].astype(jnp.float32) + xin[j, :, columns].astype(jnp.float32)
        ).astype(jnp.bfloat16)
        z_outs[j, h] = send(
            part(zout.at[j - 1], h),
            part(zin.at[j - 1], h),
            rs.at[j - 1, h],
            rr.at[j - 1, h],
            line[j - 1],
        )

    shared_copy = []

    def SH(j, h):
        arrived(y_rows, (0, 0), (0, 1))
        loaded(2, 5)
        pair = jnp.concatenate([normed_ref[...], rows[1, 0, 0]], axis=0)
        shared = jnp.dot(
            hidden_of(pair, sgate, sup), sdown[...], preferred_element_type=jnp.float32
        )
        sout[...] = shared[count:].astype(jnp.bfloat16)
        total[...] = stream_ref[...].astype(jnp.float32) + shared[:count]

    def SS(j, h):
        shared_copy.append(send(sout, sin, ss, sr, mirror))

    actions = {f.__name__: f for f in (RX, RY, RD, HO, HP, FD, FO, SH, SS, DR, FR)}
    by_x, by_z, steps = moe_plan()
    rows[0, 0, 0] = normed_ref[...]
    for j in slabs:
        k = depth - j
        for h in range(2):
            z_rows[j, h] = send(
                part(normed_ref, h),
                part(rows.at[0, j, 0], h),
                zs.at[k - 1, h],
                zr.at[k - 1, h],
                line[k - 1],
            )
    for step in steps:
        number = int(step[2:3] or 0)
        actions[step[:2]](number, "ab".index(step[3:4] or "a"))
    shared_copy[0].wait_recv()
    arrived(x_outs, (0, 0), (0, 1))
    value = total[...] + sin[...].astype(jnp.float32)
    value = value + parts[0, 0].astype(jnp.float32) + xin[0].astype(jnp.float32)
    for j in range(1, depth):
        arrived(z_outs, (j, 0), (j, 1))
        value = value + zin[j - 1].astype(jnp.float32)
    out_ref[...] = value.astype(out_ref.dtype)
    for copy in started:
        copy.wait_send()


def moe_plan():
    return (1, 2), (3,), [
        step
        for group in (
            "RX0a RX0b FR6 FR7",
            "RY1a RX1a RX1b RY1b",
            "RY0b RY0a RX3a RX3b",
            "RD1b RY2a DR RD1a",
            "RY2b RD3a RY3b RX2a",
            "SH RX2b HO0 RD2a",
            "RY3a RD3b RD2b HP1",
            "HO1 RD0a HP3 FD1a",
            "FD1b RD0b HO3 HP2",
            "FD3a SS FO1a HO2",
            "FD3b FO1b FD2b FO3a",
            "HP0 FD2a FO3b FO2b",
            "FD0b FD0a FO2a",
        )
        for step in group.split()
    ]


def run_whole(small, large, tp, sp, collective_id):
    key, value, query, _, routes, route_weight, residual, head_gain, norm_gain = small
    count, width = residual.shape
    tokens, lanes = key.shape
    head_group = small[3].shape[0]
    depth = sp // 2
    quarter = large[1].shape[1]
    half = 2 * quarter
    bf16, f32 = jnp.bfloat16, jnp.float32
    vmem = pl.BlockSpec(memory_space=pltpu.VMEM)
    pieces = 8
    table = (sp, -(-count // 128) * 128)

    def dma(*shape):
        return [pltpu.SemaphoreType.DMA(shape)] * 2

    maps = 2 * head_group
    scratch = [
        ((depth, 2, tokens, lanes), bf16),
        ((depth, 2, tokens, value.shape[1]), bf16),
        ((maps, tokens, lanes), bf16),
        ((maps, tokens, 1), f32),
        ((maps, tokens, 1), f32),
        ((maps, tokens, value.shape[1]), f32),
        ((head_group, tokens, value.shape[1]), bf16),
        ((tp * head_group, count, value.shape[1]), bf16),
        (large[0].shape, bf16),
        ((count, width), bf16),
        ((count, width), bf16),
        ((sp,) + table, f32),
        ((width, half), bf16),
        ((width, half), bf16),
        ((2 * half, width), bf16),
        ((width, half), bf16),
        ((width, half), bf16),
        ((half, width), bf16),
        ((2, depth, 2, count, width), bf16),
        ((depth, 2 * count, half), bf16),
        ((depth, 2 * count, half), bf16),
        ((depth, 2 * count, half), bf16),
        ((depth, 2, count, width), bf16),
        ((depth, count, width), bf16),
        ((depth - 1, count, width), bf16),
        ((depth - 1, count, width), bf16),
        ((count, width), bf16),
        ((count, width), bf16),
        ((count, width), f32),
    ]
    return pl.pallas_call(
        partial(whole_kernel, sp, tp),
        out_shape=jax.ShapeDtypeStruct((count, width), bf16),
        in_specs=[pl.BlockSpec(memory_space=pltpu.HBM)] * (len(small) + len(large)),
        out_specs=vmem,
        scratch_shapes=[
            pltpu.VMEM(query.shape, bf16),
            pltpu.SMEM(small[3].shape, f32),
            pltpu.VMEM(routes.shape, jnp.int32),
            pltpu.VMEM(route_weight.shape, f32),
            pltpu.VMEM(residual.shape, bf16),
            pltpu.VMEM(head_gain.shape, f32),
            pltpu.VMEM(norm_gain.shape, f32),
            pltpu.VMEM(table, f32),
        ]
        + [pltpu.VMEM(shape, dtype) for shape, dtype in scratch]
        + dma(depth - 1, 2)
        + dma(depth, 2)
        + dma(2 * depth, 2)
        + dma(depth)
        + dma(depth, 2)
        + dma(depth - 1, 2)
        + [pltpu.SemaphoreType.DMA] * 2
        + dma(2, depth - 1)
        + dma(2, depth)
        + dma(tp - 1)
        + dma(6)
        + dma(pieces)
        + dma(pieces)
        + dma(sp - 1)
        + [pltpu.SemaphoreType.DMA((len(large),)), pltpu.SemaphoreType.DMA((len(small),))],
        compiler_params=pltpu.CompilerParams(
            collective_id=collective_id,
            has_side_effects=True,
            vmem_limit_bytes=56 * 1024 * 1024,
        ),
        cost_estimate=pl.CostEstimate(
            flops=12 * depth * count * width * half * 3,
            bytes_accessed=30_000_000,
            transcendentals=0,
        ),
    )(*small, *large)


def dense_body(
    query_maps,
    key_maps,
    value_rows,
    mix_lambda,
    head_gain,
    out_weight,
    residual,
    norm_gain,
    routes,
    route_weight,
    expert_gate,
    expert_up,
    expert_down,
    shared_gate,
    shared_up,
    shared_down,
):
    sp = lax.axis_size("sp")
    tp = lax.axis_size("tp")
    return run_whole(
        (
            key_maps,
            value_rows,
            query_maps,
            mix_lambda,
            routes.T,
            route_weight.T,
            residual,
            head_gain.reshape(1, -1),
            norm_gain.reshape(1, -1),
        ),
        (
            out_weight,
            expert_gate[0],
            expert_up[0],
            shared_gate,
            shared_up,
            shared_down,
            expert_down[0],
        ),
        tp,
        sp,
        1,
    )


def solution(mesh):
    in_specs = (
        P("sp", "tp"),
        P("sp", "tp"),
        P("sp", "tp"),
        P("tp"),
        P(),
        P(),
        P(("sp", "tp"), None),
        P(),
        P("sp", None),
        P(("sp", "tp"), None),
        P("sp", None, "tp"),
        P("sp", None, "tp"),
        P("sp", "tp", None),
        P(None, "tp"),
        P(None, "tp"),
        P("tp", None),
    )
    out_specs = P(("sp", "tp"), None)
    sp, tp = mesh.shape["sp"], mesh.shape["tp"]

    def chosen(*args):
        route_count = args[8].shape[1]
        experts = sp * args[10].shape[0]
        rows_dev = args[6].shape[0]
        whole_blocks = 2 * rows_dev * route_count >= experts * rows_dev
        kv_local = args[2].shape[1] // args[4].shape[0]
        dense = whole_blocks and args[10].shape[0] == 1 and sp == 8 and tp == 4 and kv_local == 1
        if not dense:
            return body(*args)
        return dense_body(*args)

    return jax.shard_map(
        chosen, mesh=mesh, in_specs=in_specs, out_specs=out_specs, check_vma=False
    )
```

```python
import math
from functools import partial

import jax
import jax.numpy as jnp
from jax import lax
from jax.experimental import pallas as pl
from jax.experimental.pallas import tpu as pltpu
from jax.sharding import PartitionSpec as P

norm_eps = 1e-06
lowest_score = -1e30


def slot_targets(block_routes, experts, capacity):
    flat_routes = block_routes.reshape(-1)
    onehot = (flat_routes[:, None] == jnp.arange(experts, dtype=jnp.int32)[None, :]).astype(
        jnp.int32
    )
    earlier = jnp.cumsum(onehot, axis=0) - onehot
    return flat_routes * capacity + jnp.sum(earlier * onehot, axis=1)


def build_buffer(token_rows, block_routes, experts, capacity):
    targets = slot_targets(block_routes, experts, capacity)
    row_total = block_routes.shape[0]
    route_count = block_routes.shape[1]
    source_row = jnp.arange(row_total * route_count, dtype=jnp.int32) // route_count
    holder = jnp.full((experts * capacity,), row_total, jnp.int32).at[targets].set(source_row)
    padded = jnp.concatenate(
        [token_rows, jnp.zeros((1, token_rows.shape[1]), token_rows.dtype)], axis=0
    )
    return (padded[holder], targets)


def attention_block(carried, queries, key_block, value_block, score_scale):
    run_max, run_sum, accumulated = carried
    kv_local = run_max.shape[0]
    key_heads = key_block.reshape(key_block.shape[0], kv_local, 2, -1)
    value_heads = value_block.reshape(value_block.shape[0], kv_local, -1)
    scores = (
        jnp.einsum("qagcd,racd->agcqr", queries, key_heads, preferred_element_type=jnp.float32)
        * score_scale
    )
    new_max = jnp.maximum(run_max, jnp.max(scores, axis=-1))
    rescale = jnp.exp(run_max - new_max)
    weights = jnp.exp(scores - new_max[..., None])
    run_sum = run_sum * rescale + jnp.sum(weights, axis=-1)
    update = jnp.einsum(
        "agcqr,rae->agcqe",
        weights.astype(jnp.bfloat16),
        value_heads,
        preferred_element_type=jnp.float32,
    )
    return (new_max, run_sum, accumulated * rescale[..., None] + update)


def fold_keys(carried, pieces, first_row, queries, score_scale):
    key_piece, value_piece = pieces
    total_rows = key_piece.shape[0]
    block_rows = total_rows
    for candidate in (2048, 1024, 512):
        if total_rows % candidate == 0:
            block_rows = candidate
            break
    block_count = total_rows // block_rows

    def block_step(block_index, running):
        start_row = block_index * block_rows
        return attention_block(
            running,
            queries,
            lax.dynamic_slice_in_dim(key_piece, start_row, block_rows, 0),
            lax.dynamic_slice_in_dim(value_piece, start_row, block_rows, 0),
            score_scale,
        )

    return lax.fori_loop(0, block_count, block_step, carried)


def whole_experts(arrived, whole_gate, whole_up, whole_down, senders, capacity, groups):
    local_experts = whole_gate.shape[0]
    width = arrived.shape[-1]
    rows_in = arrived.reshape(senders, local_experts, capacity, width)
    gate_value = jnp.einsum(
        "sjtd,jdf->sjtf", rows_in, whole_gate, preferred_element_type=jnp.float32
    )
    up_value = jnp.einsum("sjtd,jdf->sjtf", rows_in, whole_up, preferred_element_type=jnp.float32)
    hidden = (jax.nn.silu(gate_value) * up_value).astype(jnp.bfloat16)
    hidden_units = hidden.shape[-1]
    hidden = hidden.reshape(senders, local_experts, capacity, groups, hidden_units // groups)
    down_groups = whole_down.reshape(local_experts, groups, hidden_units // groups, width)
    group_sums = jnp.einsum(
        "sjtgf,jgfd->sjtgd", hidden, down_groups, preferred_element_type=jnp.float32
    )
    group_sums = lax.optimization_barrier(group_sums.astype(jnp.bfloat16)).astype(jnp.float32)
    return (
        jnp.sum(group_sums, axis=3)
        .astype(jnp.bfloat16)
        .reshape(senders * local_experts * capacity, width)
    )


def body(
    query_maps,
    key_maps,
    value_rows,
    mix_lambda,
    head_gain,
    out_weight,
    residual,
    norm_gain,
    routes,
    route_weight,
    expert_gate,
    expert_up,
    expert_down,
    shared_gate,
    shared_up,
    shared_down,
):
    local_heads = mix_lambda.shape[0]
    head_width = head_gain.shape[0]
    kv_local = value_rows.shape[1] // head_width
    head_group = local_heads // kv_local
    head_dim = key_maps.shape[1] // (2 * kv_local)
    token_count = query_maps.shape[0]
    queries = query_maps.reshape(token_count, kv_local, head_group, 2, head_dim)
    start_max = jnp.full((kv_local, head_group, 2, token_count), lowest_score, jnp.float32)
    start_sum = jnp.zeros((kv_local, head_group, 2, token_count), jnp.float32)
    start_values = jnp.zeros((kv_local, head_group, 2, token_count, head_width), jnp.float32)
    folder = partial(fold_keys, queries=queries, score_scale=head_dim ** (-0.5))
    _, run_sum, accumulated = folder(
        (start_max, start_sum, start_values),
        (
            lax.all_gather(key_maps, "sp", axis=0, tiled=True),
            lax.all_gather(value_rows, "sp", axis=0, tiled=True),
        ),
        jnp.int32(0),
    )
    normalized = accumulated / run_sum[..., None]
    lambdas = mix_lambda.reshape(kv_local, head_group, 1, 1)
    difference = normalized[:, :, 0] - lambdas * normalized[:, :, 1]
    inverse_rms = lax.rsqrt(jnp.mean(difference * difference, axis=-1, keepdims=True) + norm_eps)
    head_scaled = (difference * inverse_rms * head_gain).astype(jnp.bfloat16)
    attended = jnp.transpose(head_scaled, (2, 0, 1, 3)).reshape(
        token_count, local_heads * head_width
    )
    columns = lax.axis_size("tp")
    column = lax.axis_index("tp")
    rows_dev = token_count // columns
    own_rows = lax.dynamic_slice_in_dim(
        out_weight, column * attended.shape[1], attended.shape[1], 0
    )
    projected = lax.psum_scatter(
        jnp.dot(attended, own_rows, preferred_element_type=jnp.float32).astype(jnp.bfloat16),
        "tp",
        scatter_dimension=0,
        tiled=True,
    ).astype(jnp.float32)
    stream = (residual.astype(jnp.float32) + projected).astype(jnp.bfloat16)
    stream_wide = stream.astype(jnp.float32)
    stream_rms = lax.rsqrt(jnp.mean(stream_wide * stream_wide, axis=1, keepdims=True) + norm_eps)
    normed = (stream_wide * stream_rms * norm_gain).astype(jnp.bfloat16)
    senders = lax.axis_size("sp")
    local_experts = expert_gate.shape[0]
    experts = senders * local_experts
    route_count = routes.shape[1]
    capacity = max(2, 2 * rows_dev * route_count // experts)
    local_routed = None
    whole_gate, whole_up, whole_down = (
        lax.all_gather(expert_gate, "tp", axis=2, tiled=True),
        lax.all_gather(expert_up, "tp", axis=2, tiled=True),
        lax.all_gather(expert_down, "tp", axis=1, tiled=True),
    )
    own_routes = lax.dynamic_slice_in_dim(routes, column * rows_dev, rows_dev, 0)
    buffer, targets = build_buffer(normed, own_routes, experts, capacity)
    arrived = lax.all_to_all(buffer, "sp", split_axis=0, concat_axis=0, tiled=True)
    local_routed = whole_experts(
        arrived, whole_gate, whole_up, whole_down, senders, capacity, columns
    )
    shared_rows = lax.all_gather(normed[None], "tp", axis=0, tiled=True)
    shared_in = shared_rows
    shared_in = shared_in.reshape(1 * lax.axis_size("tp") * rows_dev, shared_in.shape[-1])
    shared_hidden = (
        jax.nn.silu(jnp.dot(shared_in, shared_gate, preferred_element_type=jnp.float32))
        * jnp.dot(shared_in, shared_up, preferred_element_type=jnp.float32)
    ).astype(jnp.bfloat16)
    shared_out = jnp.dot(shared_hidden, shared_down, preferred_element_type=jnp.float32)
    pieces = shared_out.reshape(1 * lax.axis_size("tp"), rows_dev, shared_out.shape[-1])
    terms_out = pieces.astype(jnp.bfloat16)
    summed = (
        lax.psum_scatter(
            lax.optimization_barrier(terms_out).astype(jnp.float32).astype(jnp.bfloat16),
            "tp",
            scatter_dimension=0,
            tiled=True,
        )
        .astype(jnp.float32)[0]
        .astype(jnp.bfloat16)
    )
    returned = lax.all_to_all(local_routed, "sp", split_axis=0, concat_axis=0, tiled=True)
    picked = (
        returned[targets].reshape(rows_dev, route_count, returned.shape[-1]).astype(jnp.float32)
    )
    routed_sum = jnp.sum(route_weight[:, :, None] * picked, axis=1)
    return (stream_wide + summed.astype(jnp.float32) + routed_sum).astype(jnp.bfloat16)


MESH = pl.DeviceIdType.MESH


def remote(src, dst, send_sem, recv_sem, peer):
    return pltpu.make_async_remote_copy(
        src_ref=src,
        dst_ref=dst,
        send_sem=send_sem,
        recv_sem=recv_sem,
        device_id=peer,
        device_id_type=MESH,
    )


def grid_place(sp):
    s = lax.axis_index("sp")
    t = lax.axis_index("tp")
    return s, t, s // 2, s % 2, sp // 2


def whole_kernel(sp, tp, *refs):
    inputs, small = refs[:9], refs[17:25]
    out_weight, own_gate, own_up, own_sgate, own_sup, own_sdown, own_down = refs[9:16]
    out_ref = refs[16]
    query_ref, lam_ref, routes_ref, route_weight_ref = small[:4]
    residual_ref, head_gain_ref, norm_gain_ref, table_ref = small[4:]
    kbuf, vbuf, qbuf, run_max, run_acc, att_out, att_in, proj = refs[25:33]
    normed_ref, stream_ref, tab_in = refs[33:36]
    gate, up, down, sgate, sup, sdown = refs[36:42]
    rows, hid_own, hid_out, hid_in, parts, xin, zout, zin, sout, sin, total = refs[42:53]
    zs, zr, xs, xr, ys, yr, hs, hr, os_, or_, rs, rr, ss, sr = refs[53:67]
    kzs, kzr, kxs, kxr, hes, her, ns, nr, fs, fr, gs, gr, ts, tr, wsem, isem = refs[67:]
    s, t, z, x, depth = grid_place(sp)
    count, width = normed_ref.shape
    quarter = own_gate.shape[1]
    tokens, lanes = kbuf.shape[2:]
    head_group = lam_ref.shape[0]
    y, c = t // 2, t % 2
    across = (z * 2 + (1 - x), t)
    mirror = (s, (1 - y) * 2 + c)
    partner = (s, y * 2 + 1 - c)
    opposite = (s, (1 - y) * 2 + 1 - c)
    levels = [z, z + 1 - 2 * (z % 2), lax.rem(z + 2, depth), depth - 1 - z]
    inner = (z > 0) & (z < depth - 1)
    line = [(level * 2 + x, t) for level in levels]
    far_line = [(level * 2 + 1 - x, t) for level in levels]
    first, second = pl.ds(0, quarter), pl.ds(quarter, quarter)
    started, inner_started = [], []

    def send(source, target, send_sem, recv_sem, peer):
        copy = remote(source, target, send_sem, recv_sem, peer)
        copy.start()
        started.append(copy)
        return copy

    def inner_send(describe, *key):
        remote(*describe(*key)).start()
        inner_started.append((describe, key))

    relays = {1: (3, 2), 3: (1, 2), 2: (1, 3)}

    loads = [
        pltpu.make_async_copy(source, place, wsem.at[n])
        for n, (source, place) in enumerate(
            (
                (own_gate, gate.at[:, first]),
                (own_up, up.at[:, first]),
                (own_sgate, sgate.at[:, first]),
                (own_sup, sup.at[:, first]),
                (own_sdown, sdown.at[first]),
                (own_down, down.at[first]),
                (out_weight, proj),
            )
        )
    ]
    peers = line[1:] + far_line[1:] + [across, mirror, partner, opposite]
    barrier = pltpu.get_barrier_semaphore()
    for peer in peers:
        pl.semaphore_signal(barrier, inc=1, device_id=peer, device_id_type=MESH)
    fetches = [
        pltpu.make_async_copy(source, place, isem.at[n])
        for n, (source, place) in enumerate(
            zip(
                inputs,
                (
                    kbuf.at[0, 0],
                    vbuf.at[0, 0],
                    query_ref,
                    lam_ref,
                    routes_ref,
                    route_weight_ref,
                    residual_ref,
                    head_gain_ref,
                    norm_gain_ref,
                ),
            )
        )
    ]
    for fetch in fetches:
        fetch.start()
    fetches[0].wait()
    fetches[1].wait()
    pl.semaphore_wait(barrier, len(peers))
    keys_x = {}

    def send_keys_x(j):
        keys_x[j] = [
            send(buf.at[j, 0], buf.at[j, 1], kxs.at[i, j], kxr.at[i, j], across)
            for i, buf in enumerate((kbuf, vbuf))
        ]

    kv = (kbuf, vbuf)

    def key_copy(i, source, target, peer):
        return (
            kv[i].at[source, 0],
            kv[i].at[target, 0],
            kzs.at[i, peer, target - 1],
            kzr.at[i, target - 1],
            line[peer],
        )

    def wait_keys(m):
        for i in range(2):
            remote(*key_copy(i, 0, m, 1)).wait_recv()

    for i in range(2):
        send(*key_copy(i, 0, 1, 1))

    @pl.when(inner)
    def _():
        for i in range(2):
            inner_send(key_copy, i, 0, 3, 3)

    send_keys_x(0)
    for n in (6, 0, 1, 2, 3, 4, 5):
        loads[n].start()
    pieces = fs.shape[0]
    early = pieces - 2
    piece = quarter // pieces
    far_down = []

    def send_far(n):
        far_down.append(
            send(
                own_down.at[pl.ds(n * piece, piece)],
                down.at[pl.ds(2 * quarter + n * piece, piece)],
                fs.at[n],
                fr.at[n],
                mirror,
            )
        )

    send_far(0)
    send_far(1)
    near = [
        send(source, place, ns.at[n], nr.at[n], partner)
        for n, (source, place) in enumerate(
            (
                (own_gate, gate.at[:, second]),
                (own_up, up.at[:, second]),
                (own_sgate, sgate.at[:, second]),
                (own_sup, sup.at[:, second]),
                (own_sdown, sdown.at[second]),
                (own_down, down.at[second]),
            )
        )
    ]
    for fetch in fetches[2:]:
        fetch.wait()
    lane = lax.broadcasted_iota(jnp.int32, (tokens, lanes), 1)
    for a in range(head_group):
        head_query = query_ref[:, a * lanes : (a + 1) * lanes]
        for i in range(2):
            mine = (lane >= i * (lanes // 2)) & (lane < (i + 1) * (lanes // 2))
            qbuf[2 * a + i] = jnp.where(mine, head_query, jnp.zeros_like(head_query))
    scale = (lanes // 2) ** (-0.5) * math.log2(math.e)
    head_width = vbuf.shape[3]

    def attend(j, side):
        if side == 1:
            for copy in keys_x[j]:
                copy.wait_recv()
        keys = kbuf[j, side]
        ones = jnp.ones((tokens, lanes), jnp.bfloat16)
        values = jnp.concatenate([vbuf[j, side], ones], axis=1)
        for m in range(2 * head_group):
            scores = scale * lax.dot_general(
                qbuf[m], keys, (((1,), (1,)), ((), ())), preferred_element_type=jnp.float32
            )
            top = jnp.max(scores, axis=1, keepdims=True)
            if (j, side) != (0, 0):
                old = run_max[m]
                top = jnp.maximum(old, top)
                shrink = jnp.exp2(old - top)
            weights = jnp.exp2(scores - top).astype(jnp.bfloat16)
            update = jnp.dot(weights, values, preferred_element_type=jnp.float32)
            if (j, side) != (0, 0):
                update = update + run_acc[m] * shrink
            run_max[m] = top
            run_acc[m] = update

    def relay_inner(m):
        @pl.when(inner)
        def _():
            if m != 1:
                wait_keys(m)
            for i in range(2):
                inner_send(key_copy, i, m, relays[m][1], relays[m][0])

    def relay_keys(m):
        if m == 1:
            wait_keys(m)
            relay_inner(m)
        else:

            @pl.when(jnp.logical_not(inner))
            def _():
                wait_keys(m)

        send_keys_x(m)

    def build_table():
        chosen = routes_ref[:, :count]
        for n in range(1, tp):
            chosen = jnp.where(t == n, routes_ref[:, n * count : (n + 1) * count], chosen)
        names = [
            jnp.sum(
                jnp.where(chosen == expert, route_weight_ref[...], 0.0), axis=0, keepdims=True
            )
            for expert in range(sp)
        ]
        table = jnp.concatenate(names, axis=0)
        spare = jnp.zeros((sp, table_ref.shape[1] - count), jnp.float32)
        table_ref[...] = jnp.concatenate([table, spare], axis=1)
        tab_in[s] = table_ref[...]
        return [
            send(table_ref, tab_in.at[s], ts.at[n], tr.at[n], peer)
            for n, peer in enumerate(line[1:] + far_line[1:] + [across])
        ]

    attend(0, 0)
    relay_keys(1)
    relay_inner(3)
    send_far(2)
    attend(0, 1)
    relay_inner(2)
    attend(1, 0)
    relay_keys(2)
    attend(1, 1)
    send_far(3)
    attend(2, 0)
    relay_keys(3)
    tables = build_table()
    attend(3, 0)
    send_far(4)
    attend(2, 1)
    attend(3, 1)

    def mapped(m):
        return run_acc[m, :, :head_width] / run_acc[m, :, head_width:]

    for a in range(head_group):
        value = mapped(2 * a) - lam_ref[a] * mapped(2 * a + 1)
        rms = lax.rsqrt(jnp.mean(value * value, axis=1, keepdims=True) + norm_eps)
        att_out[a] = (value * rms * head_gain_ref[...]).astype(jnp.bfloat16)
    heads = [
        send(
            att_out.at[:, pl.ds(pl.multiple_of(peer[1] * count, 16), count)],
            att_in.at[pl.ds(head_group * t, head_group)],
            hes.at[n],
            her.at[n],
            peer,
        )
        for n, peer in enumerate((mirror, opposite, partner))
    ]
    for n in range(5, early):
        send_far(n)
    att_in[pl.ds(head_group * t, head_group)] = att_out[
        :, pl.ds(pl.multiple_of(t * count, 16), count)
    ]
    loads[6].wait()
    for copy in heads:
        copy.wait_recv()
    attended = jnp.concatenate([att_in[h] for h in range(tp * head_group)], axis=1)
    stream = (
        residual_ref[...].astype(jnp.float32)
        + jnp.dot(attended, proj[...], preferred_element_type=jnp.float32)
    ).astype(jnp.bfloat16)
    stream_ref[...] = stream
    wide = stream.astype(jnp.float32)
    inverse = lax.rsqrt(jnp.mean(wide * wide, axis=1, keepdims=True) + norm_eps)
    normed_ref[...] = (wide * inverse * norm_gain_ref[...]).astype(jnp.bfloat16)

    x_rows, y_rows, diagonal, hids, x_outs, z_outs = {}, {}, {}, {}, {}, {}
    half_width = width // 2
    waited = set()

    def part(ref, h):
        return ref.at[:, pl.ds(h * half_width, half_width)]

    def own_rows(j, h):
        return part(normed_ref if j == 0 else rows.at[0, j, 0], h)

    def hidden_of(block, gate_buf, up_buf):
        gate_value = jnp.dot(block, gate_buf[...], preferred_element_type=jnp.float32)
        up_value = jnp.dot(block, up_buf[...], preferred_element_type=jnp.float32)
        return (jax.nn.silu(gate_value) * up_value).astype(jnp.bfloat16)

    def arrived(copies, *keys):
        for key in keys:
            if (id(copies), key) not in waited:
                waited.add((id(copies), key))
                copies[key].wait_recv()

    def loaded(first_load, last_load):
        for n in range(first_load, last_load):
            if ("load", n) not in waited:
                waited.add(("load", n))
                loads[n].wait()
                near[n].wait_recv()

    def level_copy(source, target, peer, h):
        return (
            own_rows(source, h),
            part(rows.at[0, target, 0], h),
            zs.at[peer, target - 1, h],
            zr.at[target - 1, h],
            line[peer],
        )

    def wait_level(m, h):
        remote(*level_copy(0, m, 1, h)).wait_recv()

    def level_arrived(m, h):
        if ("level", m, h) not in waited:
            waited.add(("level", m, h))
            if m == 1:
                wait_level(m, h)
            else:

                @pl.when(jnp.logical_not(inner))
                def _():
                    wait_level(m, h)

    def ZF(m, h):
        if m == 1:
            level_arrived(m, h)

        @pl.when(inner)
        def _():
            if m != 1:
                wait_level(m, h)
            inner_send(level_copy, m, relays[m][1], relays[m][0], h)

    def RX(j, h):
        if j != 0:
            level_arrived(j, h)
        x_rows[j, h] = send(
            own_rows(j, h), part(rows.at[0, j, 1], h), xs.at[j, h], xr.at[j, h], across
        )

    def RY(j, h):
        sems = ys.at[j, h], yr.at[j, h]
        if j in by_z:
            arrived(y_rows, (0, h))
            y_rows[j, h] = send(
                part(rows.at[1, 0, 0], h), part(rows.at[1, j, 0], h), *sems, line[j]
            )
            return
        if j != 0:
            level_arrived(j, h)
        y_rows[j, h] = send(own_rows(j, h), part(rows.at[1, j, 0], h), *sems, mirror)

    def RD(j, h):
        sems = ys.at[depth + j, h], yr.at[depth + j, h]
        target = part(rows.at[1, j, 1], h)
        if j in by_x:
            arrived(y_rows, (j, h))
            diagonal[j, h] = send(part(rows.at[1, j, 0], h), target, *sems, across)
        else:
            arrived(x_rows, (j, h))
            diagonal[j, h] = send(part(rows.at[0, j, 1], h), target, *sems, mirror)

    def HO(j, h):
        if j != 0:
            level_arrived(j, 0)
            level_arrived(j, 1)
        arrived(x_rows, (j, 0), (j, 1))
        loaded(0, 2)
        hid_own[j] = hidden_of(rows[0, j].reshape(2 * count, width), gate, up)

    def HP(j, h):
        arrived(y_rows, (j, 0), (j, 1))
        arrived(diagonal, (j, 0), (j, 1))
        loaded(0, 2)
        hid_out[j] = hidden_of(rows[1, j].reshape(2 * count, width), gate, up)
        hids[j] = send(hid_out.at[j], hid_in.at[j], hs.at[j], hr.at[j], mirror)

    far_near = []

    def FR(j, h):
        for n in range(j, pieces):
            if n == j or h:
                send_far(n)

    def DR(j, h):
        for n, copy in enumerate(far_down):
            copy.wait_recv()
            far_near.append(
                send(
                    down.at[pl.ds(2 * quarter + n * piece, piece)],
                    down.at[pl.ds(3 * quarter + n * piece, piece)],
                    gs.at[n],
                    gr.at[n],
                    partner,
                )
            )

    def route_column(source):
        row = tab_in[source, pl.ds(s, 1)]
        shape = (count, row.shape[1])
        diagonal_mask = lax.broadcasted_iota(jnp.int32, shape, 0) == lax.broadcasted_iota(
            jnp.int32, shape, 1
        )
        spread = jnp.broadcast_to(row, shape)
        return jnp.sum(jnp.where(diagonal_mask, spread, 0.0), axis=1, keepdims=True)

    def FD(j, h):
        loaded(5, 6)
        for copies in (far_near, tables):
            if ("all", id(copies)) not in waited:
                waited.add(("all", id(copies)))
                for copy in copies:
                    copy.wait_recv()
        arrived(hids, j)
        half = hid_own.shape[2]
        columns = pl.ds(h * half_width, half_width)
        value = jnp.dot(
            hid_own[j], down[pl.ds(0, half), columns], preferred_element_type=jnp.float32
        ) + jnp.dot(
            hid_in[j], down[pl.ds(half, half), columns], preferred_element_type=jnp.float32
        )
        base = levels[j] * 2
        parts[j, 1, :, columns] = (value[count:] * route_column(base + 1 - x)).astype(
            jnp.bfloat16
        )
        x_outs[j, h] = send(
            part(parts.at[j, 1], h), part(xin.at[j], h), os_.at[j, h], or_.at[j, h], across
        )
        parts[j, 0, :, columns] = (value[:count] * route_column(base + x)).astype(jnp.bfloat16)

    def FO(j, h):
        arrived(x_outs, (j, h))
        columns = pl.ds(h * half_width, half_width)
        zout[j - 1, :, columns] = (
            parts[j, 0, :, columns].astype(jnp.float32) + xin[j, :, columns].astype(jnp.float32)
        ).astype(jnp.bfloat16)
        z_outs[j, h] = send(
            part(zout.at[j - 1], h),
            part(zin.at[j - 1], h),
            rs.at[j - 1, h],
            rr.at[j - 1, h],
            line[j],
        )

    shared_copy = []

    def SH(j, h):
        arrived(y_rows, (0, 0), (0, 1))
        loaded(2, 5)
        pair = jnp.concatenate([normed_ref[...], rows[1, 0, 0]], axis=0)
        shared = jnp.dot(
            hidden_of(pair, sgate, sup), sdown[...], preferred_element_type=jnp.float32
        )
        sout[...] = shared[count:].astype(jnp.bfloat16)
        total[...] = stream_ref[...].astype(jnp.float32) + shared[:count]

    def SS(j, h):
        shared_copy.append(send(sout, sin, ss, sr, mirror))

    actions = {f.__name__: f for f in (RX, RY, RD, HO, HP, FD, FO, SH, SS, DR, FR, ZF)}
    by_x, by_z, steps = moe_plan()
    rows[0, 0, 0] = normed_ref[...]
    for h in range(2):
        send(*level_copy(0, 1, 1, h))

    @pl.when(inner)
    def _():
        for h in range(2):
            inner_send(level_copy, 0, 3, 3, h)

    for step in steps:
        number = int(step[2:3] or 0)
        actions[step[:2]](number, "ab".index(step[3:4] or "a"))
    shared_copy[0].wait_recv()
    arrived(x_outs, (0, 0), (0, 1))
    value = total[...] + sin[...].astype(jnp.float32)
    value = value + parts[0, 0].astype(jnp.float32) + xin[0].astype(jnp.float32)
    for j in range(1, depth):
        arrived(z_outs, (j, 0), (j, 1))
        value = value + zin[j - 1].astype(jnp.float32)
    out_ref[...] = value.astype(out_ref.dtype)
    for copy in started:
        copy.wait_send()

    @pl.when(inner)
    def _():
        for describe, key in inner_started:
            remote(*describe(*key)).wait_send()


def moe_plan():
    return (0, 2, 3), (1,), [
        step
        for group in (
            "RX0b RY0b FR6 RY0a",
            "RX0a FR7 RD0b ZF1a",
            "ZF3a RX1a ZF1b ZF3b",
            "RX1b ZF2a RY2a RX2a",
            "ZF2b RX2b RY2b RY1a",
            "RY3a RD2a RD2b RY3b",
            "RD1b HO2 RD3a HO0",
            "RD3b DR RX3a RY1b",
            "HP2 HO1 RD1a RX3b",
            "HP3 FD2b FD2a HP1",
            "HO3 RD0a FO2b FD3b",
            "FD1b FO2a SH FD3a",
            "FO3b FD1a HP0 SS",
            "FO1b FO3a FD0a FO1a",
            "FD0b",
        )
        for step in group.split()
    ]


def run_whole(small, large, tp, sp, collective_id):
    key, value, query, _, routes, route_weight, residual, head_gain, norm_gain = small
    count, width = residual.shape
    tokens, lanes = key.shape
    head_group = small[3].shape[0]
    depth = sp // 2
    quarter = large[1].shape[1]
    half = 2 * quarter
    bf16, f32 = jnp.bfloat16, jnp.float32
    vmem = pl.BlockSpec(memory_space=pltpu.VMEM)
    pieces = 8
    table = (sp, -(-count // 128) * 128)

    def dma(*shape):
        return [pltpu.SemaphoreType.DMA(shape)] * 2

    maps = 2 * head_group
    scratch = [
        ((depth, 2, tokens, lanes), bf16),
        ((depth, 2, tokens, value.shape[1]), bf16),
        ((maps, tokens, lanes), bf16),
        ((maps, tokens, 1), f32),
        ((maps, tokens, value.shape[1] + lanes), f32),
        ((head_group, tokens, value.shape[1]), bf16),
        ((tp * head_group, count, value.shape[1]), bf16),
        (large[0].shape, bf16),
        ((count, width), bf16),
        ((count, width), bf16),
        ((sp,) + table, f32),
        ((width, half), bf16),
        ((width, half), bf16),
        ((2 * half, width), bf16),
        ((width, half), bf16),
        ((width, half), bf16),
        ((half, width), bf16),
        ((2, depth, 2, count, width), bf16),
        ((depth, 2 * count, half), bf16),
        ((depth, 2 * count, half), bf16),
        ((depth, 2 * count, half), bf16),
        ((depth, 2, count, width), bf16),
        ((depth, count, width), bf16),
        ((depth - 1, count, width), bf16),
        ((depth - 1, count, width), bf16),
        ((count, width), bf16),
        ((count, width), bf16),
        ((count, width), f32),
    ]
    return pl.pallas_call(
        partial(whole_kernel, sp, tp),
        out_shape=jax.ShapeDtypeStruct((count, width), bf16),
        in_specs=[pl.BlockSpec(memory_space=pltpu.HBM)] * (len(small) + len(large)),
        out_specs=vmem,
        scratch_shapes=[
            pltpu.VMEM(query.shape, bf16),
            pltpu.SMEM(small[3].shape, f32),
            pltpu.VMEM(routes.shape, jnp.int32),
            pltpu.VMEM(route_weight.shape, f32),
            pltpu.VMEM(residual.shape, bf16),
            pltpu.VMEM(head_gain.shape, f32),
            pltpu.VMEM(norm_gain.shape, f32),
            pltpu.VMEM(table, f32),
        ]
        + [pltpu.VMEM(shape, dtype) for shape, dtype in scratch]
        + [pltpu.SemaphoreType.DMA((depth, depth - 1, 2)), pltpu.SemaphoreType.DMA((depth - 1, 2))]
        + dma(depth, 2)
        + dma(2 * depth, 2)
        + dma(depth)
        + dma(depth, 2)
        + dma(depth - 1, 2)
        + [pltpu.SemaphoreType.DMA] * 2
        + [pltpu.SemaphoreType.DMA((2, depth, depth - 1)), pltpu.SemaphoreType.DMA((2, depth - 1))]
        + dma(2, depth)
        + dma(tp - 1)
        + dma(6)
        + dma(pieces)
        + dma(pieces)
        + dma(sp - 1)
        + [pltpu.SemaphoreType.DMA((len(large),)), pltpu.SemaphoreType.DMA((len(small),))],
        compiler_params=pltpu.CompilerParams(
            collective_id=collective_id,
            has_side_effects=True,
            vmem_limit_bytes=56 * 1024 * 1024,
        ),
        cost_estimate=pl.CostEstimate(
            flops=12 * depth * count * width * half * 3,
            bytes_accessed=30_000_000,
            transcendentals=0,
        ),
    )(*small, *large)


def dense_body(
    query_maps,
    key_maps,
    value_rows,
    mix_lambda,
    head_gain,
    out_weight,
    residual,
    norm_gain,
    routes,
    route_weight,
    expert_gate,
    expert_up,
    expert_down,
    shared_gate,
    shared_up,
    shared_down,
):
    sp = lax.axis_size("sp")
    tp = lax.axis_size("tp")
    return run_whole(
        (
            key_maps,
            value_rows,
            query_maps,
            mix_lambda,
            routes.T,
            route_weight.T,
            residual,
            head_gain.reshape(1, -1),
            norm_gain.reshape(1, -1),
        ),
        (
            out_weight,
            expert_gate[0],
            expert_up[0],
            shared_gate,
            shared_up,
            shared_down,
            expert_down[0],
        ),
        tp,
        sp,
        1,
    )


def solution(mesh):
    in_specs = (
        P("sp", "tp"),
        P("sp", "tp"),
        P("sp", "tp"),
        P("tp"),
        P(),
        P(),
        P(("sp", "tp"), None),
        P(),
        P("sp", None),
        P(("sp", "tp"), None),
        P("sp", None, "tp"),
        P("sp", None, "tp"),
        P("sp", "tp", None),
        P(None, "tp"),
        P(None, "tp"),
        P("tp", None),
    )
    out_specs = P(("sp", "tp"), None)
    sp, tp = mesh.shape["sp"], mesh.shape["tp"]

    def chosen(*args):
        route_count = args[8].shape[1]
        experts = sp * args[10].shape[0]
        rows_dev = args[6].shape[0]
        whole_blocks = 2 * rows_dev * route_count >= experts * rows_dev
        kv_local = args[2].shape[1] // args[4].shape[0]
        dense = whole_blocks and args[10].shape[0] == 1 and sp == 8 and tp == 4 and kv_local == 1
        if not dense:
            return body(*args)
        return dense_body(*args)

    return jax.shard_map(
        chosen, mesh=mesh, in_specs=in_specs, out_specs=out_specs, check_vma=False
    )
```

```python
import math
from functools import partial

import jax
import jax.numpy as jnp
from jax import lax
from jax.experimental import pallas as pl
from jax.experimental.pallas import tpu as pltpu
from jax.sharding import PartitionSpec as P

norm_eps = 1e-06
lowest_score = -1e30


def slot_targets(block_routes, experts, capacity):
    flat_routes = block_routes.reshape(-1)
    onehot = (flat_routes[:, None] == jnp.arange(experts, dtype=jnp.int32)[None, :]).astype(
        jnp.int32
    )
    earlier = jnp.cumsum(onehot, axis=0) - onehot
    return flat_routes * capacity + jnp.sum(earlier * onehot, axis=1)


def build_buffer(token_rows, block_routes, experts, capacity):
    targets = slot_targets(block_routes, experts, capacity)
    row_total = block_routes.shape[0]
    route_count = block_routes.shape[1]
    source_row = jnp.arange(row_total * route_count, dtype=jnp.int32) // route_count
    holder = jnp.full((experts * capacity,), row_total, jnp.int32).at[targets].set(source_row)
    padded = jnp.concatenate(
        [token_rows, jnp.zeros((1, token_rows.shape[1]), token_rows.dtype)], axis=0
    )
    return (padded[holder], targets)


def attention_block(carried, queries, key_block, value_block, score_scale):
    run_max, run_sum, accumulated = carried
    kv_local = run_max.shape[0]
    key_heads = key_block.reshape(key_block.shape[0], kv_local, 2, -1)
    value_heads = value_block.reshape(value_block.shape[0], kv_local, -1)
    scores = (
        jnp.einsum("qagcd,racd->agcqr", queries, key_heads, preferred_element_type=jnp.float32)
        * score_scale
    )
    new_max = jnp.maximum(run_max, jnp.max(scores, axis=-1))
    rescale = jnp.exp(run_max - new_max)
    weights = jnp.exp(scores - new_max[..., None])
    run_sum = run_sum * rescale + jnp.sum(weights, axis=-1)
    update = jnp.einsum(
        "agcqr,rae->agcqe",
        weights.astype(jnp.bfloat16),
        value_heads,
        preferred_element_type=jnp.float32,
    )
    return (new_max, run_sum, accumulated * rescale[..., None] + update)


def fold_keys(carried, pieces, first_row, queries, score_scale):
    key_piece, value_piece = pieces
    total_rows = key_piece.shape[0]
    block_rows = total_rows
    for candidate in (2048, 1024, 512):
        if total_rows % candidate == 0:
            block_rows = candidate
            break
    block_count = total_rows // block_rows

    def block_step(block_index, running):
        start_row = block_index * block_rows
        return attention_block(
            running,
            queries,
            lax.dynamic_slice_in_dim(key_piece, start_row, block_rows, 0),
            lax.dynamic_slice_in_dim(value_piece, start_row, block_rows, 0),
            score_scale,
        )

    return lax.fori_loop(0, block_count, block_step, carried)


def whole_experts(arrived, whole_gate, whole_up, whole_down, senders, capacity, groups):
    local_experts = whole_gate.shape[0]
    width = arrived.shape[-1]
    rows_in = arrived.reshape(senders, local_experts, capacity, width)
    gate_value = jnp.einsum(
        "sjtd,jdf->sjtf", rows_in, whole_gate, preferred_element_type=jnp.float32
    )
    up_value = jnp.einsum("sjtd,jdf->sjtf", rows_in, whole_up, preferred_element_type=jnp.float32)
    hidden = (jax.nn.silu(gate_value) * up_value).astype(jnp.bfloat16)
    hidden_units = hidden.shape[-1]
    hidden = hidden.reshape(senders, local_experts, capacity, groups, hidden_units // groups)
    down_groups = whole_down.reshape(local_experts, groups, hidden_units // groups, width)
    group_sums = jnp.einsum(
        "sjtgf,jgfd->sjtgd", hidden, down_groups, preferred_element_type=jnp.float32
    )
    group_sums = lax.optimization_barrier(group_sums.astype(jnp.bfloat16)).astype(jnp.float32)
    return (
        jnp.sum(group_sums, axis=3)
        .astype(jnp.bfloat16)
        .reshape(senders * local_experts * capacity, width)
    )


def body(
    query_maps,
    key_maps,
    value_rows,
    mix_lambda,
    head_gain,
    out_weight,
    residual,
    norm_gain,
    routes,
    route_weight,
    expert_gate,
    expert_up,
    expert_down,
    shared_gate,
    shared_up,
    shared_down,
):
    local_heads = mix_lambda.shape[0]
    head_width = head_gain.shape[0]
    kv_local = value_rows.shape[1] // head_width
    head_group = local_heads // kv_local
    head_dim = key_maps.shape[1] // (2 * kv_local)
    token_count = query_maps.shape[0]
    queries = query_maps.reshape(token_count, kv_local, head_group, 2, head_dim)
    start_max = jnp.full((kv_local, head_group, 2, token_count), lowest_score, jnp.float32)
    start_sum = jnp.zeros((kv_local, head_group, 2, token_count), jnp.float32)
    start_values = jnp.zeros((kv_local, head_group, 2, token_count, head_width), jnp.float32)
    folder = partial(fold_keys, queries=queries, score_scale=head_dim ** (-0.5))
    _, run_sum, accumulated = folder(
        (start_max, start_sum, start_values),
        (
            lax.all_gather(key_maps, "sp", axis=0, tiled=True),
            lax.all_gather(value_rows, "sp", axis=0, tiled=True),
        ),
        jnp.int32(0),
    )
    normalized = accumulated / run_sum[..., None]
    lambdas = mix_lambda.reshape(kv_local, head_group, 1, 1)
    difference = normalized[:, :, 0] - lambdas * normalized[:, :, 1]
    inverse_rms = lax.rsqrt(jnp.mean(difference * difference, axis=-1, keepdims=True) + norm_eps)
    head_scaled = (difference * inverse_rms * head_gain).astype(jnp.bfloat16)
    attended = jnp.transpose(head_scaled, (2, 0, 1, 3)).reshape(
        token_count, local_heads * head_width
    )
    columns = lax.axis_size("tp")
    column = lax.axis_index("tp")
    rows_dev = token_count // columns
    own_rows = lax.dynamic_slice_in_dim(
        out_weight, column * attended.shape[1], attended.shape[1], 0
    )
    projected = lax.psum_scatter(
        jnp.dot(attended, own_rows, preferred_element_type=jnp.float32).astype(jnp.bfloat16),
        "tp",
        scatter_dimension=0,
        tiled=True,
    ).astype(jnp.float32)
    stream = (residual.astype(jnp.float32) + projected).astype(jnp.bfloat16)
    stream_wide = stream.astype(jnp.float32)
    stream_rms = lax.rsqrt(jnp.mean(stream_wide * stream_wide, axis=1, keepdims=True) + norm_eps)
    normed = (stream_wide * stream_rms * norm_gain).astype(jnp.bfloat16)
    senders = lax.axis_size("sp")
    local_experts = expert_gate.shape[0]
    experts = senders * local_experts
    route_count = routes.shape[1]
    capacity = max(2, 2 * rows_dev * route_count // experts)
    local_routed = None
    whole_gate, whole_up, whole_down = (
        lax.all_gather(expert_gate, "tp", axis=2, tiled=True),
        lax.all_gather(expert_up, "tp", axis=2, tiled=True),
        lax.all_gather(expert_down, "tp", axis=1, tiled=True),
    )
    own_routes = lax.dynamic_slice_in_dim(routes, column * rows_dev, rows_dev, 0)
    buffer, targets = build_buffer(normed, own_routes, experts, capacity)
    arrived = lax.all_to_all(buffer, "sp", split_axis=0, concat_axis=0, tiled=True)
    local_routed = whole_experts(
        arrived, whole_gate, whole_up, whole_down, senders, capacity, columns
    )
    shared_rows = lax.all_gather(normed[None], "tp", axis=0, tiled=True)
    shared_in = shared_rows
    shared_in = shared_in.reshape(1 * lax.axis_size("tp") * rows_dev, shared_in.shape[-1])
    shared_hidden = (
        jax.nn.silu(jnp.dot(shared_in, shared_gate, preferred_element_type=jnp.float32))
        * jnp.dot(shared_in, shared_up, preferred_element_type=jnp.float32)
    ).astype(jnp.bfloat16)
    shared_out = jnp.dot(shared_hidden, shared_down, preferred_element_type=jnp.float32)
    pieces = shared_out.reshape(1 * lax.axis_size("tp"), rows_dev, shared_out.shape[-1])
    terms_out = pieces.astype(jnp.bfloat16)
    summed = (
        lax.psum_scatter(
            lax.optimization_barrier(terms_out).astype(jnp.float32).astype(jnp.bfloat16),
            "tp",
            scatter_dimension=0,
            tiled=True,
        )
        .astype(jnp.float32)[0]
        .astype(jnp.bfloat16)
    )
    returned = lax.all_to_all(local_routed, "sp", split_axis=0, concat_axis=0, tiled=True)
    picked = (
        returned[targets].reshape(rows_dev, route_count, returned.shape[-1]).astype(jnp.float32)
    )
    routed_sum = jnp.sum(route_weight[:, :, None] * picked, axis=1)
    return (stream_wide + summed.astype(jnp.float32) + routed_sum).astype(jnp.bfloat16)


MESH = pl.DeviceIdType.MESH


def remote(src, dst, send_sem, recv_sem, peer):
    return pltpu.make_async_remote_copy(
        src_ref=src,
        dst_ref=dst,
        send_sem=send_sem,
        recv_sem=recv_sem,
        device_id=peer,
        device_id_type=MESH,
    )


def grid_place(sp):
    s = lax.axis_index("sp")
    t = lax.axis_index("tp")
    return s, t, s // 2, s % 2, sp // 2


def whole_kernel(sp, tp, *refs):
    inputs, small = refs[:9], refs[17:25]
    out_weight, own_gate, own_up, own_sgate, own_sup, own_sdown, own_down = refs[9:16]
    out_ref = refs[16]
    query_ref, lam_ref, routes_ref, route_weight_ref = small[:4]
    residual_ref, head_gain_ref, norm_gain_ref, table_ref = small[4:]
    kbuf, vbuf, qbuf, run_max, run_acc, att_out, att_in, proj = refs[25:33]
    normed_ref, stream_ref, tab_in = refs[33:36]
    gate, up, down, sgate, sup, sdown = refs[36:42]
    rows, hid_own, hid_out, hid_in, parts, xin, zout, zin, sout, sin, total = refs[42:53]
    zs, zr, xs, xr, ys, yr, hs, hr, os_, or_, rs, rr, ss, sr = refs[53:67]
    kzs, kzr, kxs, kxr, hes, her, ns, nr, fs, fr, gs, gr, ts, tr, wsem, isem = refs[67:]
    s, t, z, x, depth = grid_place(sp)
    count, width = normed_ref.shape
    quarter = own_gate.shape[1]
    tokens, lanes = kbuf.shape[2:]
    head_group = lam_ref.shape[0]
    y, c = t // 2, t % 2
    across = (z * 2 + (1 - x), t)
    mirror = (s, (1 - y) * 2 + c)
    partner = (s, y * 2 + 1 - c)
    opposite = (s, (1 - y) * 2 + 1 - c)
    levels = [z, z + 1 - 2 * (z % 2), lax.rem(z + 2, depth), depth - 1 - z]
    inner = (z > 0) & (z < depth - 1)
    line = [(level * 2 + x, t) for level in levels]
    far_line = [(level * 2 + 1 - x, t) for level in levels]
    first, second = pl.ds(0, quarter), pl.ds(quarter, quarter)
    started, inner_started = [], []

    def send(source, target, send_sem, recv_sem, peer):
        copy = remote(source, target, send_sem, recv_sem, peer)
        copy.start()
        started.append(copy)
        return copy

    def inner_send(describe, *key):
        remote(*describe(*key)).start()
        inner_started.append((describe, key))

    relays = {1: (3, 2), 3: (1, 2), 2: (1, 3)}

    loads = [
        pltpu.make_async_copy(source, place, wsem.at[n])
        for n, (source, place) in enumerate(
            (
                (own_gate, gate.at[:, first]),
                (own_up, up.at[:, first]),
                (own_sgate, sgate.at[:, first]),
                (own_sup, sup.at[:, first]),
                (own_sdown, sdown.at[first]),
                (own_down, down.at[first]),
                (out_weight, proj),
            )
        )
    ]
    peers = line[1:] + far_line[1:] + [across, mirror, partner, opposite]
    barrier = pltpu.get_barrier_semaphore()
    for peer in peers:
        pl.semaphore_signal(barrier, inc=1, device_id=peer, device_id_type=MESH)
    fetches = [
        pltpu.make_async_copy(source, place, isem.at[n])
        for n, (source, place) in enumerate(
            zip(
                inputs,
                (
                    kbuf.at[0, 0],
                    vbuf.at[0, 0],
                    query_ref,
                    lam_ref,
                    routes_ref,
                    route_weight_ref,
                    residual_ref,
                    head_gain_ref,
                    norm_gain_ref,
                ),
            )
        )
    ]
    for fetch in fetches:
        fetch.start()
    fetches[0].wait()
    fetches[1].wait()
    pl.semaphore_wait(barrier, len(peers))
    keys_x = {}

    def send_keys_x(j):
        keys_x[j] = [
            send(buf.at[j, 0], buf.at[j, 1], kxs.at[i, j], kxr.at[i, j], across)
            for i, buf in enumerate((kbuf, vbuf))
        ]

    kv = (kbuf, vbuf)

    def key_copy(i, source, target, peer):
        return (
            kv[i].at[source, 0],
            kv[i].at[target, 0],
            kzs.at[i, peer, target - 1],
            kzr.at[i, target - 1],
            line[peer],
        )

    def wait_keys(m):
        for i in range(2):
            remote(*key_copy(i, 0, m, 1)).wait_recv()

    for i in range(2):
        send(*key_copy(i, 0, 1, 1))

    @pl.when(inner)
    def _():
        for i in range(2):
            inner_send(key_copy, i, 0, 3, 3)

    send_keys_x(0)
    for n in (6, 0, 1, 2, 3, 4, 5):
        loads[n].start()
    pieces = fs.shape[0]
    early = pieces - 1
    piece = quarter // pieces
    far_down = []

    def send_far(n):
        far_down.append(
            send(
                own_down.at[pl.ds(n * piece, piece)],
                down.at[pl.ds(2 * quarter + n * piece, piece)],
                fs.at[n],
                fr.at[n],
                mirror,
            )
        )

    send_far(0)
    send_far(1)
    near = [
        send(source, place, ns.at[n], nr.at[n], partner)
        for n, (source, place) in enumerate(
            (
                (own_gate, gate.at[:, second]),
                (own_up, up.at[:, second]),
                (own_sgate, sgate.at[:, second]),
                (own_sup, sup.at[:, second]),
                (own_sdown, sdown.at[second]),
                (own_down, down.at[second]),
            )
        )
    ]
    for fetch in fetches[2:]:
        fetch.wait()
    lane = lax.broadcasted_iota(jnp.int32, (tokens, lanes), 1)
    for a in range(head_group):
        head_query = query_ref[:, a * lanes : (a + 1) * lanes]
        for i in range(2):
            mine = (lane >= i * (lanes // 2)) & (lane < (i + 1) * (lanes // 2))
            qbuf[2 * a + i] = jnp.where(mine, head_query, jnp.zeros_like(head_query))
    scale = (lanes // 2) ** (-0.5) * math.log2(math.e)
    head_width = vbuf.shape[3]

    def attend(j, side):
        if side == 1:
            for copy in keys_x[j]:
                copy.wait_recv()
        keys = kbuf[j, side]
        ones = jnp.ones((tokens, lanes), jnp.bfloat16)
        values = jnp.concatenate([vbuf[j, side], ones], axis=1)
        for m in range(2 * head_group):
            scores = scale * lax.dot_general(
                qbuf[m], keys, (((1,), (1,)), ((), ())), preferred_element_type=jnp.float32
            )
            top = jnp.max(scores, axis=1, keepdims=True)
            if (j, side) != (0, 0):
                old = run_max[m]
                top = jnp.maximum(old, top)
                shrink = jnp.exp2(old - top)
            weights = jnp.exp2(scores - top).astype(jnp.bfloat16)
            update = jnp.dot(weights, values, preferred_element_type=jnp.float32)
            if (j, side) != (0, 0):
                update = update + run_acc[m] * shrink
            run_max[m] = top
            run_acc[m] = update

    def relay_inner(m):
        @pl.when(inner)
        def _():
            if m != 1:
                wait_keys(m)
            for i in range(2):
                inner_send(key_copy, i, m, relays[m][1], relays[m][0])

    def relay_keys(m):
        if m == 1:
            wait_keys(m)
            relay_inner(m)
        else:

            @pl.when(jnp.logical_not(inner))
            def _():
                wait_keys(m)

        send_keys_x(m)

    def build_table():
        chosen = routes_ref[:, :count]
        for n in range(1, tp):
            chosen = jnp.where(t == n, routes_ref[:, n * count : (n + 1) * count], chosen)
        names = [
            jnp.sum(
                jnp.where(chosen == expert, route_weight_ref[...], 0.0), axis=0, keepdims=True
            )
            for expert in range(sp)
        ]
        table = jnp.concatenate(names, axis=0)
        spare = jnp.zeros((sp, table_ref.shape[1] - count), jnp.float32)
        table_ref[...] = jnp.concatenate([table, spare], axis=1)
        tab_in[s] = table_ref[...]
        return [
            send(table_ref, tab_in.at[s], ts.at[n], tr.at[n], peer)
            for n, peer in enumerate(line[1:] + far_line[1:] + [across])
        ]

    attend(0, 0)
    relay_keys(1)
    relay_inner(3)
    send_far(2)
    attend(0, 1)
    relay_inner(2)
    attend(1, 0)
    relay_keys(2)
    attend(1, 1)
    send_far(3)
    attend(2, 0)
    relay_keys(3)
    tables = build_table()
    attend(3, 0)
    send_far(4)
    attend(2, 1)
    attend(3, 1)

    def mapped(m):
        return run_acc[m, :, :head_width] / run_acc[m, :, head_width:]

    for a in range(head_group):
        value = mapped(2 * a) - lam_ref[a] * mapped(2 * a + 1)
        rms = lax.rsqrt(jnp.mean(value * value, axis=1, keepdims=True) + norm_eps)
        att_out[a] = (value * rms * head_gain_ref[...]).astype(jnp.bfloat16)
    heads = [
        send(
            att_out.at[:, pl.ds(pl.multiple_of(peer[1] * count, 16), count)],
            att_in.at[pl.ds(head_group * t, head_group)],
            hes.at[n],
            her.at[n],
            peer,
        )
        for n, peer in enumerate((mirror, opposite, partner))
    ]
    for n in range(5, early):
        send_far(n)
    att_in[pl.ds(head_group * t, head_group)] = att_out[
        :, pl.ds(pl.multiple_of(t * count, 16), count)
    ]
    loads[6].wait()
    for copy in heads:
        copy.wait_recv()
    attended = jnp.concatenate([att_in[h] for h in range(tp * head_group)], axis=1)
    stream = (
        residual_ref[...].astype(jnp.float32)
        + jnp.dot(attended, proj[...], preferred_element_type=jnp.float32)
    ).astype(jnp.bfloat16)
    stream_ref[...] = stream
    wide = stream.astype(jnp.float32)
    inverse = lax.rsqrt(jnp.mean(wide * wide, axis=1, keepdims=True) + norm_eps)
    normed_ref[...] = (wide * inverse * norm_gain_ref[...]).astype(jnp.bfloat16)

    x_rows, y_rows, diagonal, hids, x_outs, z_outs = {}, {}, {}, {}, {}, {}
    half_width = width // 2
    waited = set()

    def part(ref, h):
        return ref.at[:, pl.ds(h * half_width, half_width)]

    def own_rows(j, h):
        return part(normed_ref if j == 0 else rows.at[0, j, 0], h)

    def hidden_of(block, gate_buf, up_buf):
        gate_value = jnp.dot(block, gate_buf[...], preferred_element_type=jnp.float32)
        up_value = jnp.dot(block, up_buf[...], preferred_element_type=jnp.float32)
        return (jax.nn.silu(gate_value) * up_value).astype(jnp.bfloat16)

    def arrived(copies, *keys):
        for key in keys:
            if (id(copies), key) not in waited:
                waited.add((id(copies), key))
                copies[key].wait_recv()

    def loaded(first_load, last_load):
        for n in range(first_load, last_load):
            if ("load", n) not in waited:
                waited.add(("load", n))
                loads[n].wait()
                near[n].wait_recv()

    def level_copy(source, target, peer, h):
        return (
            own_rows(source, h),
            part(rows.at[0, target, 0], h),
            zs.at[peer, target - 1, h],
            zr.at[target - 1, h],
            line[peer],
        )

    def wait_level(m, h):
        remote(*level_copy(0, m, 1, h)).wait_recv()

    def level_arrived(m, h):
        if ("level", m, h) not in waited:
            waited.add(("level", m, h))
            if m == 1:
                wait_level(m, h)
            else:

                @pl.when(jnp.logical_not(inner))
                def _():
                    wait_level(m, h)

    def ZF(m, h):
        if m == 1:
            level_arrived(m, h)

        @pl.when(inner)
        def _():
            if m != 1:
                wait_level(m, h)
            inner_send(level_copy, m, relays[m][1], relays[m][0], h)

    def RX(j, h):
        if j in by_zx:
            arrived(x_rows, (0, h))
            x_rows[j, h] = send(
                part(rows.at[0, 0, 1], h),
                part(rows.at[0, j, 1], h),
                xs.at[j, h],
                xr.at[j, h],
                line[j],
            )
            return
        if j != 0:
            level_arrived(j, h)
        x_rows[j, h] = send(
            own_rows(j, h), part(rows.at[0, j, 1], h), xs.at[j, h], xr.at[j, h], across
        )

    def RY(j, h):
        sems = ys.at[j, h], yr.at[j, h]
        if j in by_z:
            arrived(y_rows, (0, h))
            y_rows[j, h] = send(
                part(rows.at[1, 0, 0], h), part(rows.at[1, j, 0], h), *sems, line[j]
            )
            return
        if j != 0:
            level_arrived(j, h)
        y_rows[j, h] = send(own_rows(j, h), part(rows.at[1, j, 0], h), *sems, mirror)

    def RD(j, h):
        sems = ys.at[depth + j, h], yr.at[depth + j, h]
        target = part(rows.at[1, j, 1], h)
        if j in by_zd:
            arrived(diagonal, (0, h))
            diagonal[j, h] = send(part(rows.at[1, 0, 1], h), target, *sems, line[j])
        elif j in by_x:
            arrived(y_rows, (j, h))
            diagonal[j, h] = send(part(rows.at[1, j, 0], h), target, *sems, across)
        else:
            arrived(x_rows, (j, h))
            diagonal[j, h] = send(part(rows.at[0, j, 1], h), target, *sems, mirror)

    def HO(j, h):
        if j != 0:
            level_arrived(j, 0)
            level_arrived(j, 1)
        arrived(x_rows, (j, 0), (j, 1))
        loaded(0, 2)
        hid_own[j] = hidden_of(rows[0, j].reshape(2 * count, width), gate, up)

    def HP(j, h):
        arrived(y_rows, (j, 0), (j, 1))
        arrived(diagonal, (j, 0), (j, 1))
        loaded(0, 2)
        hid_out[j] = hidden_of(rows[1, j].reshape(2 * count, width), gate, up)
        hids[j] = send(hid_out.at[j], hid_in.at[j], hs.at[j], hr.at[j], mirror)

    far_near = []

    def FR(j, h):
        for n in range(j, pieces):
            if n == j or h:
                send_far(n)

    def DR(j, h):
        for n, copy in enumerate(far_down):
            copy.wait_recv()
            far_near.append(
                send(
                    down.at[pl.ds(2 * quarter + n * piece, piece)],
                    down.at[pl.ds(3 * quarter + n * piece, piece)],
                    gs.at[n],
                    gr.at[n],
                    partner,
                )
            )

    def route_column(source):
        row = tab_in[source, pl.ds(s, 1)]
        shape = (count, row.shape[1])
        diagonal_mask = lax.broadcasted_iota(jnp.int32, shape, 0) == lax.broadcasted_iota(
            jnp.int32, shape, 1
        )
        spread = jnp.broadcast_to(row, shape)
        return jnp.sum(jnp.where(diagonal_mask, spread, 0.0), axis=1, keepdims=True)

    def FD(j, h):
        loaded(5, 6)
        for copies in (far_near, tables):
            if ("all", id(copies)) not in waited:
                waited.add(("all", id(copies)))
                for copy in copies:
                    copy.wait_recv()
        arrived(hids, j)
        half = hid_own.shape[2]
        columns = pl.ds(h * half_width, half_width)
        value = jnp.dot(
            hid_own[j], down[pl.ds(0, half), columns], preferred_element_type=jnp.float32
        ) + jnp.dot(
            hid_in[j], down[pl.ds(half, half), columns], preferred_element_type=jnp.float32
        )
        base = levels[j] * 2
        parts[j, 1, :, columns] = (value[count:] * route_column(base + 1 - x)).astype(
            jnp.bfloat16
        )
        x_outs[j, h] = send(
            part(parts.at[j, 1], h), part(xin.at[j], h), os_.at[j, h], or_.at[j, h], across
        )
        parts[j, 0, :, columns] = (value[:count] * route_column(base + x)).astype(jnp.bfloat16)

    def FO(j, h):
        arrived(x_outs, (j, h))
        columns = pl.ds(h * half_width, half_width)
        zout[j - 1, :, columns] = (
            parts[j, 0, :, columns].astype(jnp.float32) + xin[j, :, columns].astype(jnp.float32)
        ).astype(jnp.bfloat16)
        z_outs[j, h] = send(
            part(zout.at[j - 1], h),
            part(zin.at[j - 1], h),
            rs.at[j - 1, h],
            rr.at[j - 1, h],
            line[j],
        )

    shared_copy = []

    def SH(j, h):
        arrived(y_rows, (0, 0), (0, 1))
        loaded(2, 5)
        pair = jnp.concatenate([normed_ref[...], rows[1, 0, 0]], axis=0)
        shared = jnp.dot(
            hidden_of(pair, sgate, sup), sdown[...], preferred_element_type=jnp.float32
        )
        sout[...] = shared[count:].astype(jnp.bfloat16)
        total[...] = stream_ref[...].astype(jnp.float32) + shared[:count]

    def SS(j, h):
        shared_copy.append(send(sout, sin, ss, sr, mirror))

    actions = {f.__name__: f for f in (RX, RY, RD, HO, HP, FD, FO, SH, SS, DR, FR, ZF)}
    by_x, (by_z, by_zx, by_zd), steps = moe_plan()
    rows[0, 0, 0] = normed_ref[...]
    for h in range(2):
        send(*level_copy(0, 1, 1, h))

    @pl.when(inner)
    def _():
        for h in range(2):
            inner_send(level_copy, 0, 3, 3, h)

    for step in steps:
        number = int(step[2:3] or 0)
        actions[step[:2]](number, "ab".index(step[3:4] or "a"))
    shared_copy[0].wait_recv()
    arrived(x_outs, (0, 0), (0, 1))
    value = total[...] + sin[...].astype(jnp.float32)
    value = value + parts[0, 0].astype(jnp.float32) + xin[0].astype(jnp.float32)
    for j in range(1, depth):
        arrived(z_outs, (j, 0), (j, 1))
        value = value + zin[j - 1].astype(jnp.float32)
    out_ref[...] = value.astype(out_ref.dtype)
    for copy in started:
        copy.wait_send()

    @pl.when(inner)
    def _():
        for describe, key in inner_started:
            remote(*describe(*key)).wait_send()


def moe_plan():
    return (2, 3), ((1,), (1,), (1,)), [
        step
        for group in (
            "RX0b FR7 RX0a RY0a",
            "RY0b ZF1a ZF3a ZF2a",
            "RY2a RX2a ZF1b ZF3b",
            "ZF2b RY2b RX2b RX1a",
            "RY1a RY3a RD0a RD2a",
            "RD0b RY3b RD2b RY1b",
            "RX3a HO2 SH DR",
            "RD3a HP2 RX3b HP0",
            "RD3b RD1a HO0 RD1b",
            "SS FD2b FD2a HP3",
            "RX1b FD0a FO2b HO3",
            "HP1 FD3b FO2a FD3a",
            "HO1 FD1b FO3b FD1a",
            "FD0b FO3a FO1b FO1a",
        )
        for step in group.split()
    ]


def run_whole(small, large, tp, sp, collective_id):
    key, value, query, _, routes, route_weight, residual, head_gain, norm_gain = small
    count, width = residual.shape
    tokens, lanes = key.shape
    head_group = small[3].shape[0]
    depth = sp // 2
    quarter = large[1].shape[1]
    half = 2 * quarter
    bf16, f32 = jnp.bfloat16, jnp.float32
    vmem = pl.BlockSpec(memory_space=pltpu.VMEM)
    pieces = 8
    table = (sp, -(-count // 128) * 128)

    def dma(*shape):
        return [pltpu.SemaphoreType.DMA(shape)] * 2

    maps = 2 * head_group
    scratch = [
        ((depth, 2, tokens, lanes), bf16),
        ((depth, 2, tokens, value.shape[1]), bf16),
        ((maps, tokens, lanes), bf16),
        ((maps, tokens, 1), f32),
        ((maps, tokens, value.shape[1] + lanes), f32),
        ((head_group, tokens, value.shape[1]), bf16),
        ((tp * head_group, count, value.shape[1]), bf16),
        (large[0].shape, bf16),
        ((count, width), bf16),
        ((count, width), bf16),
        ((sp,) + table, f32),
        ((width, half), bf16),
        ((width, half), bf16),
        ((2 * half, width), bf16),
        ((width, half), bf16),
        ((width, half), bf16),
        ((half, width), bf16),
        ((2, depth, 2, count, width), bf16),
        ((depth, 2 * count, half), bf16),
        ((depth, 2 * count, half), bf16),
        ((depth, 2 * count, half), bf16),
        ((depth, 2, count, width), bf16),
        ((depth, count, width), bf16),
        ((depth - 1, count, width), bf16),
        ((depth - 1, count, width), bf16),
        ((count, width), bf16),
        ((count, width), bf16),
        ((count, width), f32),
    ]
    return pl.pallas_call(
        partial(whole_kernel, sp, tp),
        out_shape=jax.ShapeDtypeStruct((count, width), bf16),
        in_specs=[pl.BlockSpec(memory_space=pltpu.HBM)] * (len(small) + len(large)),
        out_specs=vmem,
        scratch_shapes=[
            pltpu.VMEM(query.shape, bf16),
            pltpu.SMEM(small[3].shape, f32),
            pltpu.VMEM(routes.shape, jnp.int32),
            pltpu.VMEM(route_weight.shape, f32),
            pltpu.VMEM(residual.shape, bf16),
            pltpu.VMEM(head_gain.shape, f32),
            pltpu.VMEM(norm_gain.shape, f32),
            pltpu.VMEM(table, f32),
        ]
        + [pltpu.VMEM(shape, dtype) for shape, dtype in scratch]
        + [pltpu.SemaphoreType.DMA((depth, depth - 1, 2)), pltpu.SemaphoreType.DMA((depth - 1, 2))]
        + dma(depth, 2)
        + dma(2 * depth, 2)
        + dma(depth)
        + dma(depth, 2)
        + dma(depth - 1, 2)
        + [pltpu.SemaphoreType.DMA] * 2
        + [pltpu.SemaphoreType.DMA((2, depth, depth - 1)), pltpu.SemaphoreType.DMA((2, depth - 1))]
        + dma(2, depth)
        + dma(tp - 1)
        + dma(6)
        + dma(pieces)
        + dma(pieces)
        + dma(sp - 1)
        + [pltpu.SemaphoreType.DMA((len(large),)), pltpu.SemaphoreType.DMA((len(small),))],
        compiler_params=pltpu.CompilerParams(
            collective_id=collective_id,
            has_side_effects=True,
            vmem_limit_bytes=56 * 1024 * 1024,
        ),
        cost_estimate=pl.CostEstimate(
            flops=12 * depth * count * width * half * 3,
            bytes_accessed=30_000_000,
            transcendentals=0,
        ),
    )(*small, *large)


def dense_body(
    query_maps,
    key_maps,
    value_rows,
    mix_lambda,
    head_gain,
    out_weight,
    residual,
    norm_gain,
    routes,
    route_weight,
    expert_gate,
    expert_up,
    expert_down,
    shared_gate,
    shared_up,
    shared_down,
):
    sp = lax.axis_size("sp")
    tp = lax.axis_size("tp")
    return run_whole(
        (
            key_maps,
            value_rows,
            query_maps,
            mix_lambda,
            routes.T,
            route_weight.T,
            residual,
            head_gain.reshape(1, -1),
            norm_gain.reshape(1, -1),
        ),
        (
            out_weight,
            expert_gate[0],
            expert_up[0],
            shared_gate,
            shared_up,
            shared_down,
            expert_down[0],
        ),
        tp,
        sp,
        1,
    )


def solution(mesh):
    in_specs = (
        P("sp", "tp"),
        P("sp", "tp"),
        P("sp", "tp"),
        P("tp"),
        P(),
        P(),
        P(("sp", "tp"), None),
        P(),
        P("sp", None),
        P(("sp", "tp"), None),
        P("sp", None, "tp"),
        P("sp", None, "tp"),
        P("sp", "tp", None),
        P(None, "tp"),
        P(None, "tp"),
        P("tp", None),
    )
    out_specs = P(("sp", "tp"), None)
    sp, tp = mesh.shape["sp"], mesh.shape["tp"]

    def chosen(*args):
        route_count = args[8].shape[1]
        experts = sp * args[10].shape[0]
        rows_dev = args[6].shape[0]
        whole_blocks = 2 * rows_dev * route_count >= experts * rows_dev
        kv_local = args[2].shape[1] // args[4].shape[0]
        dense = whole_blocks and args[10].shape[0] == 1 and sp == 8 and tp == 4 and kv_local == 1
        if not dense:
            return body(*args)
        return dense_body(*args)

    return jax.shard_map(
        chosen, mesh=mesh, in_specs=in_specs, out_specs=out_specs, check_vma=False
    )
```
